128 devices in a mesh: sp: 16 (over z, x), tp: 8 (over y, core).
Axes of the slice: x: 4, y: 4, z: 4, core: 2. Of those that a mesh axis runs over, the one named last changes fastest.
Arguments:
- query_wide: bfloat16 [12288, 8, 256], P('sp', 'tp'), may hold values from -6 to 6
- key_wide: bfloat16 [12288, 8, 256], P('sp', 'tp'), may hold values from -6 to 6
- value_wide: bfloat16 [12288, 8, 256], P('sp', 'tp'), may hold values from -6 to 6
- query_narrow: bfloat16 [12288, 8, 128], P('sp', 'tp'), may hold values from -6 to 6
- key_narrow: bfloat16 [12288, 8, 128], P('sp', 'tp'), may hold values from -6 to 6
- value_narrow: bfloat16 [12288, 8, 128], P('sp', 'tp'), may hold values from -6 to 6
- mix_lambda: float32 [2, 8], P(None, 'tp'), may hold values from 0.3 to 0.8
- residual_in: bfloat16 [12288, 2048], P(('sp', 'tp')), may hold values from -6 to 6
- out_wide: bfloat16 [2048, 2048], P('tp'), may hold values from -0.109375 to 0.109375
- out_narrow: bfloat16 [1024, 2048], P('tp'), may hold values from -0.109375 to 0.109375
- ffn_gain: float32 [2048], replicated, may hold values from 0.1 to 1.9
- expert_ids: int32 [12288, 2], P(('sp', 'tp')), may hold values from 0 to 127, as said below
- expert_weights: float32 [12288, 2], P(('sp', 'tp')), may hold values from 0.1 to 1
- gate_weight: bfloat16 [128, 2048, 1024], P(('sp', 'tp')), may hold values from -0.125 to 0.125
- up_weight: bfloat16 [128, 2048, 1024], P(('sp', 'tp')), may hold values from -0.125 to 0.125
- down_weight: bfloat16 [128, 1024, 2048], P(('sp', 'tp')), may hold values from -0.1875 to 0.1875
Outputs:
- layer_out: bfloat16 [12288, 2048], P(('sp', 'tp'))
The draws below stay inside these ranges and needn't reach their ends.
Inputs may be any that keep to these rules, and one draw needn't show every extreme that they name: `expert_ids`: A row's two experts differ and lie in the same group of 4 consecutive experts (32 groups). In each aligned block of 96 rows (the rows of one device) no expert is named by more than 3 rows, and in every block some expert is named by exactly 3 rows.
All inputs are finite; a program needn't handle non-finite values.
Results may differ from the reference program's by a relative error of at most 0.015.
Values may be sent and summed in bfloat16 or wider, within the bound.
A program may use at most 192 MiB of HBM per device.

```python
import math
import jax
import jax.numpy as jnp
from jax import lax

D = 2048
HEADS = 8
DA = 128
DB = 64
VA = 256
VB = 128
FF = 1024
GROUP_SIZE = 4
TOKENS = 12288
TOK_LOC = 96
EXPERTS = 128
CAP = 3


def query_draw(key, salt, head_size):
    values_drawn = jnp.clip(jax.random.normal(jax.random.fold_in(key, salt + 100), (TOKENS, HEADS, 2 * head_size), jnp.float32) * 1.3, -6.0, 6.0)
    return values_drawn.astype(jnp.bfloat16)


def key_draw(key, salt, head_size):
    values_drawn = jnp.clip(jax.random.normal(jax.random.fold_in(key, salt + 200), (TOKENS, HEADS, 2 * head_size), jnp.float32) * 1.3, -6.0, 6.0)
    return values_drawn.astype(jnp.bfloat16)


def draw_query_wide(key, part):
    return query_draw(key, 5, DA)


def draw_key_wide(key, part):
    return key_draw(key, 5, DA)


def draw_query_narrow(key, part):
    return query_draw(key, 9, DB)


def draw_key_narrow(key, part):
    return key_draw(key, 9, DB)


def draw_expert_ids(key, part):
    positions = EXPERTS * CAP // 2
    blocks = TOKENS // TOK_LOC
    forced = jax.random.randint(jax.random.fold_in(key, 31), (), 0, EXPERTS)
    pair_first = jnp.array([[0, 2], [0, 1], [0, 1]], jnp.int32)
    pair_second = jnp.array([[1, 3], [2, 3], [3, 2]], jnp.int32)

    def one_block(block_key):
        key_kind, key_score, key_order, key_flip = jax.random.split(block_key, 4)
        position = jnp.arange(positions, dtype=jnp.int32)
        group_index = position // (2 * CAP)
        level_index = position % (2 * CAP) // 2
        which_pair = position % 2
        pair_kind = jax.random.randint(key_kind, (EXPERTS // GROUP_SIZE, CAP), 0, 3)
        kinds = pair_kind[group_index, level_index]
        first_expert = pair_first[kinds, which_pair] + group_index * GROUP_SIZE
        second_expert = pair_second[kinds, which_pair] + group_index * GROUP_SIZE
        hit = ((first_expert == forced) | (second_expert == forced)).astype(jnp.int32)
        priority = jax.random.randint(key_score, (positions,), 0, 2 ** 20) * 1024 + position + hit * 2 ** 30
        _, chosen = lax.top_k(priority, TOK_LOC)
        shuffle = jax.random.permutation(key_order, TOK_LOC)
        picked = chosen[shuffle]
        flipped = jax.random.randint(key_flip, (TOK_LOC,), 0, 2)
        left_expert = first_expert[picked]
        right_expert = second_expert[picked]
        low_expert = jnp.where(flipped == 1, right_expert, left_expert)
        high_expert = jnp.where(flipped == 1, left_expert, right_expert)
        return jnp.stack([low_expert, high_expert], axis=-1)
    block_keys = jax.random.split(jax.random.fold_in(key, 32), blocks)
    return jax.vmap(one_block)(block_keys).reshape(TOKENS, 2).astype(jnp.int32)


def steps_of(stream_key, dims, cuts, smallest, top_value):
    gain, own = 1.0, jax.random.fold_in(stream_key, 6)
    for dim, shards_of in cuts:
        steps = jnp.exp(jax.random.uniform(jax.random.fold_in(own, dim), (shards_of,), jnp.float32, smallest / len(cuts), top_value / len(cuts)))
        gain = gain * jnp.repeat(steps, dims[dim] // shards_of).reshape([-1 if axis == dim else 1 for axis in range(len(dims))])
    return gain


def centred(stream_key, dims, spread, reach, pieces=(), kind=jnp.bfloat16):
    values = spread * jax.random.normal(stream_key, dims, jnp.float32)
    if pieces:
        values = values * steps_of(stream_key, dims, pieces, -0.22, 0.18)
    return jnp.clip(values, -reach, reach).astype(kind)


def setup_inputs(seed: int = 0) -> dict:
    streams_of = jax.random.split(jax.random.key(seed), 17)
    return {
        "query_wide": draw_query_wide(jax.random.fold_in(streams_of[16], 71), 0),
        "key_wide": draw_key_wide(jax.random.fold_in(streams_of[16], 71), 0),
        "value_wide": centred(streams_of[2], (TOKENS, HEADS, VA), 1.0, 6.0, ((0, 16), (1, 8))),
        "query_narrow": draw_query_narrow(jax.random.fold_in(streams_of[16], 71), 0),
        "key_narrow": draw_key_narrow(jax.random.fold_in(streams_of[16], 71), 0),
        "value_narrow": centred(streams_of[5], (TOKENS, HEADS, VB), 1.0, 6.0, ((0, 16), (1, 8))),
        "mix_lambda": jnp.clip(0.3 + 0.5 * jax.random.uniform(streams_of[6], (2, HEADS), jnp.float32) ** steps_of(streams_of[6], (2, HEADS), ((1, 8),), -0.2, 0.2), 0.3, 0.8),
        "residual_in": centred(streams_of[7], (TOKENS, D), 1.0, 6.0, ((0, 128),)),
        "out_wide": centred(streams_of[8], (HEADS * VA, D), (HEADS * VA + HEADS * VB) ** -0.5, 0.109375, ((0, 8),)),
        "out_narrow": centred(streams_of[9], (HEADS * VB, D), (HEADS * VA + HEADS * VB) ** -0.5, 0.109375, ((0, 8),)),
        "ffn_gain": jnp.clip(1.0 + 0.18 * jax.random.normal(streams_of[10], (D,), jnp.float32), 0.1, 1.9),
        "expert_ids": draw_expert_ids(jax.random.fold_in(streams_of[16], 71), 0),
        "expert_weights": jnp.clip(0.1 + 0.9 * jax.random.uniform(streams_of[12], (TOKENS, 2), jnp.float32) ** steps_of(streams_of[12], (TOKENS, 2), ((0, 128),), -0.2, 0.2), 0.1, 1.0),
        "gate_weight": centred(streams_of[13], (EXPERTS, D, FF), D ** -0.5, 0.125, ((0, 128),)),
        "up_weight": centred(streams_of[14], (EXPERTS, D, FF), D ** -0.5, 0.125, ((0, 128),)),
        "down_weight": centred(streams_of[15], (EXPERTS, FF, D), FF ** -0.5, 0.1875, ((0, 128),)),
    }


def head_group(query, keys, values, lam_row, head_size):
    score_scale = head_size ** (-0.5)
    query_block = math.gcd(TOKENS, 512)
    query_f = query.astype(jnp.float32)
    keys_f = keys.astype(jnp.float32)
    values_f = values.astype(jnp.float32)
    key_pos = jnp.arange(TOKENS, dtype=jnp.int32)

    def block_read(number):
        query_rows = lax.dynamic_slice_in_dim(query_f, number * query_block, query_block, 0)
        query_pos = number * query_block + jnp.arange(query_block, dtype=jnp.int32)
        causal = key_pos[None, :] <= query_pos[:, None]
        reads = []
        for which_map in range(2):
            lower_edge = which_map * head_size
            scores = jnp.einsum('qhd,khd->hqk', query_rows[..., lower_edge:lower_edge + head_size], keys_f[..., lower_edge:lower_edge + head_size]) * score_scale
            scores = jnp.where(causal[None], scores, -jnp.inf)
            new_peak = lax.optimization_barrier(jnp.max(scores, axis=-1, keepdims=True))
            expo = jnp.exp(scores - new_peak)
            totals = lax.optimization_barrier(jnp.sum(expo, axis=-1))
            rounded = lax.optimization_barrier(expo.astype(jnp.bfloat16)).astype(jnp.float32)
            reads.append(jnp.einsum('hqk,khv->hqv', rounded, values_f) / totals[..., None])
        mixed_read = reads[0] - lam_row[:, None, None] * reads[1]
        normed = mixed_read * lax.rsqrt(lax.optimization_barrier(jnp.mean(mixed_read * mixed_read, axis=-1, keepdims=True)) + 1e-06)
        return jnp.transpose(normed.astype(jnp.bfloat16), (1, 0, 2))
    outputs = lax.map(block_read, jnp.arange(TOKENS // query_block, dtype=jnp.int32))
    return outputs.reshape(TOKENS, -1)

def reference(query_wide, key_wide, value_wide, query_narrow, key_narrow, value_narrow, mix_lambda, residual_in, out_wide, out_narrow, ffn_gain, expert_ids, expert_weights, gate_weight, up_weight, down_weight):
    heads_wide = head_group(query_wide, key_wide, value_wide, mix_lambda[0], DA)
    heads_narrow = head_group(query_narrow, key_narrow, value_narrow, mix_lambda[1], DB)
    projected = jnp.dot(heads_wide, out_wide, preferred_element_type=jnp.float32) + jnp.dot(heads_narrow, out_narrow, preferred_element_type=jnp.float32)
    stream = (projected + residual_in.astype(jnp.float32)).astype(jnp.bfloat16)
    stream_f = stream.astype(jnp.float32)
    normed = (stream_f * lax.rsqrt(lax.optimization_barrier(jnp.mean(stream_f * stream_f, axis=-1, keepdims=True)) + 1e-06) * ffn_gain).astype(jnp.bfloat16)
    flat_expert = expert_ids.reshape(-1)
    flat_token = jnp.repeat(jnp.arange(TOKENS, dtype=jnp.int32), 2)
    flat_weight = expert_weights.reshape(-1)
    slots = EXPERTS * CAP

    def one_expert(running, expert):
        chosen = flat_expert == expert
        count = jnp.sum(chosen.astype(jnp.int32))
        position = jnp.nonzero(chosen, size=slots, fill_value=0)[0].astype(jnp.int32)
        token_rows = flat_token[position]
        rows = normed[token_rows]
        gate_part = jnp.dot(rows, gate_weight[expert], preferred_element_type=jnp.float32)
        up_part = jnp.dot(rows, up_weight[expert], preferred_element_type=jnp.float32)
        hidden = (jax.nn.silu(gate_part) * up_part).astype(jnp.bfloat16)
        result = jnp.dot(hidden, down_weight[expert], preferred_element_type=jnp.float32)
        result = lax.optimization_barrier(result.astype(jnp.bfloat16)).astype(jnp.float32)
        share = jnp.where(jnp.arange(slots, dtype=jnp.int32) < count, flat_weight[position], 0.0)
        return (running.at[token_rows].add(share[:, None] * result), None)
    summed, _ = lax.scan(one_expert, jnp.zeros((TOKENS, D), jnp.float32), jnp.arange(EXPERTS, dtype=jnp.int32))
    return (stream_f + summed).astype(jnp.bfloat16)
```

```python
import functools
import jax
import jax.numpy as jnp
from jax import lax
from jax.experimental import pallas as pl
from jax.experimental.pallas import tpu as pltpu
from jax.sharding import Mesh
from jax.sharding import PartitionSpec as P

TP = ("y", "c")
SP = ("z", "x")
SP_TP = ("z", "x", "y", "c")

NEG = -1e30
LOG2E = 1.4426950408889634


TQ = 256


def flash_body(pos_ref, *refs, d, dv, nq, nk):
    q_in = refs[:nq]
    kv_in = refs[nq:nq + nk]
    acc_out, stat_out = refs[nq + nk:nq + nk + 2]
    q_s, k_s, v_s, qt_s, vt_s, s_a, s_b, t_a, t_b, p_scr, acc, m_s, l_s, st_buf, tab, sems, out_sem = refs[nq + nk + 2:]
    rows = q_in[0].shape[0]
    half = rows // 2
    copies = []
    for n, src in enumerate(q_in):
        copies.append(pltpu.make_async_copy(src, q_s.at[pl.ds(n * rows, rows)], sems.at[n]))
    for n, src in enumerate(kv_in):
        for h in range(2):
            at = h * nk * half + n * half
            part = src.at[pl.ds(h * half, half)]
            copies.append(pltpu.make_async_copy(part.at[:, pl.ds(0, 2 * d)], k_s.at[pl.ds(at, half)], sems.at[nq + 4 * n + 2 * h]))
            copies.append(pltpu.make_async_copy(part.at[:, pl.ds(2 * d, dv)], v_s.at[pl.ds(at, half)], sems.at[nq + 4 * n + 2 * h + 1]))
    for c in copies:
        c.start()
    for c in copies:
        c.wait()
    scale = d ** (-0.5) * LOG2E
    total_q, total_k = nq * rows, nk * rows
    TK = rows
    tiles_q, tiles_k = total_q // TQ, total_k // TK

    def turn(i, _):
        r = pl.multiple_of(i * rows, rows)
        qt_s[:, pl.ds(r, rows)] = q_s[pl.ds(r, rows)].T
        vt_s[:, pl.ds(r, rows)] = v_s[pl.ds(r, rows)].T
        return 0
    lax.fori_loop(0, nq, turn, 0)

    def list_q(qi, n):
        per = rows // TQ
        qp = pos_ref[qi // per] + (qi % per) * TQ

        def list_k(kj, carry):
            n, first = carry
            p0, p1 = pos_ref[nq + 2 * kj], pos_ref[nq + 2 * kj + 1]
            hi, lo = jnp.maximum(p0, p1), jnp.minimum(p0, p1)
            full = hi + half - 1 <= qp
            some = lo <= qp + TQ - 1
            tab[0, n] = qi
            tab[1, n] = kj
            tab[2, n] = jnp.where(full, 0, 1)
            tab[3, n] = first
            return n + some.astype(jnp.int32), jnp.where(some, 0, first)
        m, first = lax.fori_loop(0, tiles_k, list_k, (n, 1))

        @pl.when(m == n)
        def _():
            tab[0, n] = qi
            tab[1, n] = 0
            tab[2, n] = 1
            tab[3, n] = 1
        return jnp.maximum(m, n + 1)
    steps = lax.fori_loop(0, tiles_q, list_q, 0)
    tab[3, steps] = 1

    CH = 256

    def read(i, s_buf, t_buf):
        q0 = pl.multiple_of(tab[0, i] * TQ, TQ)
        k0 = pl.multiple_of(tab[1, i] * TK, TK)
        for w in range(2):
            qt = qt_s[w * d:(w + 1) * d, pl.ds(q0, TQ)]
            top = None
            for c in range(TK // CH):
                k = k_s[pl.ds(k0 + c * CH, CH), w * d:(w + 1) * d]
                s = jnp.dot(k, qt, preferred_element_type=jnp.float32)
                s_buf[w, c * CH:(c + 1) * CH] = s
                m8 = jnp.max(s.reshape(CH // 8, 8, TQ), axis=0)
                top = m8 if top is None else jnp.maximum(top, m8)
            t_buf[w] = top

    def mask(i, s_buf, t_buf):
        per = rows // TQ
        qi, kj = tab[0, i], tab[1, i]
        qp = pos_ref[qi // per] + (qi % per) * TQ
        CM = 128
        t_buf[...] = jnp.full_like(t_buf, NEG)

        def chunk(c, _):
            r = pl.multiple_of(c * CM, CM)
            late = (c >= half // CM).astype(jnp.int32)
            k0 = pos_ref[nq + 2 * kj + late] + (c - late * (half // CM)) * CM
            keep = lax.broadcasted_iota(jnp.int32, (CM, TQ), 0) - lax.broadcasted_iota(jnp.int32, (CM, TQ), 1) <= qp - k0
            for w in range(2):
                s = jnp.where(keep, s_buf[w, pl.ds(r, CM)], NEG)
                s_buf[w, pl.ds(r, CM)] = s
                t_buf[w] = jnp.maximum(t_buf[w], jnp.max(s.reshape(CM // 8, 8, TQ), axis=0))
            return 0
        lax.fori_loop(0, TK // CM, chunk, 0)

    def weigh(i, par, s_buf, t_buf):
        k0 = pl.multiple_of(tab[1, i] * TK, TK)
        for w in range(2):
            old = m_s[w:w + 1]
            new = jnp.maximum(old, jnp.max(t_buf[w], axis=0, keepdims=True) * scale)
            f = jnp.exp2(old - new)
            m_s[w:w + 1] = new
            tot = None
            for c in range(TK // CH):
                p = jnp.exp2(s_buf[w, c * CH:(c + 1) * CH] * scale - new)
                t8 = jnp.sum(p.reshape(CH // 8, 8, TQ), axis=0)
                tot = t8 if tot is None else tot + t8
                p_scr[w, c * CH:(c + 1) * CH] = p.astype(jnp.bfloat16)
            o = jnp.dot(vt_s[:, pl.ds(k0, TK)], p_scr[w], preferred_element_type=jnp.float32)
            l_s[w] = l_s[w] * f + tot
            acc[par, w] = acc[par, w] * f + o

    def out_copies(qi, par):
        q0 = pl.multiple_of(qi * TQ, TQ)
        return (
            pltpu.make_async_copy(acc.at[par], acc_out.at[:, :, pl.ds(q0, TQ)], out_sem.at[par, 0]),
            pltpu.make_async_copy(st_buf.at[par], stat_out.at[:, pl.ds(q0, TQ)], out_sem.at[par, 1]),
        )

    def advance(i, cur, nxt):
        qi = tab[0, i]
        par = qi % 2

        @pl.when(tab[3, i] == 1)
        def _():
            @pl.when(qi >= 2)
            def _():
                for c in out_copies(qi - 2, par):
                    c.wait()
            m_s[...] = jnp.full_like(m_s, NEG)
            l_s[...] = jnp.zeros_like(l_s)
            acc[par] = jnp.zeros((2, dv, TQ), jnp.float32)

        @pl.when(tab[2, i] == 1)
        def _():
            mask(i, *cur)
        read(jnp.minimum(i + 1, steps - 1), *nxt)
        weigh(i, par, *cur)

        @pl.when(tab[3, i + 1] == 1)
        def _():
            st_buf[par, 0:2] = m_s[...]
            for w in range(2):
                st_buf[par, 2 + w:3 + w] = jnp.sum(l_s[w], axis=0, keepdims=True)
            for c in out_copies(qi, par):
                c.start()

    one, two = (s_a, t_a), (s_b, t_b)
    read(0, *one)

    def pair(n, _):
        advance(2 * n, one, two)

        @pl.when(2 * n + 1 < steps)
        def _():
            advance(2 * n + 1, two, one)
        return 0
    lax.fori_loop(0, (steps + 1) // 2, pair, 0)
    for qi in (tiles_q - 2, tiles_q - 1):
        for c in out_copies(qi, qi % 2):
            c.wait()


def flash(pos, qs, kvs, d, dv, units=9.5):
    rows = qs[0].shape[0]
    nq, nk = len(qs), len(kvs)
    total, keys = nq * rows, nk * rows
    any_ = pl.BlockSpec(memory_space=pl.ANY)
    flops = int(units * rows * rows * 2 * (d + dv) * 2)
    return pl.pallas_call(
        functools.partial(flash_body, d=d, dv=dv, nq=nq, nk=nk),
        out_shape=(jax.ShapeDtypeStruct((2, dv, total), jnp.float32), jax.ShapeDtypeStruct((4, total), jnp.float32)),
        in_specs=[pl.BlockSpec(memory_space=pltpu.SMEM)] + [any_] * (nq + nk),
        out_specs=(any_, any_),
        scratch_shapes=[
            pltpu.VMEM((total, 2 * d), jnp.bfloat16),
            pltpu.VMEM((keys, 2 * d), jnp.bfloat16),
            pltpu.VMEM((keys, dv), jnp.bfloat16),
            pltpu.VMEM((2 * d, total), jnp.bfloat16),
            pltpu.VMEM((dv, keys), jnp.bfloat16),
            pltpu.VMEM((2, rows, TQ), jnp.float32),
            pltpu.VMEM((2, rows, TQ), jnp.float32),
            pltpu.VMEM((2, 8, TQ), jnp.float32),
            pltpu.VMEM((2, 8, TQ), jnp.float32),
            pltpu.VMEM((2, rows, TQ), jnp.bfloat16),
            pltpu.VMEM((2, 2, dv, TQ), jnp.float32),
            pltpu.VMEM((2, TQ), jnp.float32),
            pltpu.VMEM((2, 8, TQ), jnp.float32),
            pltpu.VMEM((2, 4, TQ), jnp.float32),
            pltpu.SMEM((4, total // TQ * (keys // rows) + 1), jnp.int32),
            pltpu.SemaphoreType.DMA((nq + 4 * nk,)),
            pltpu.SemaphoreType.DMA((2, 2)),
        ],
        name="flash_wide" if d == 128 else "flash_narrow",
        cost_estimate=pl.CostEstimate(flops=flops, bytes_accessed=total * (dv * 8 + 2 * d * 4 + dv * 2), transcendentals=0),
        compiler_params=pltpu.CompilerParams(vmem_limit_bytes=50 * 2**20),
    )(pos, *qs, *kvs)


def mix_body(lam_ref, acc_ref, own_ref, *refs, row):
    peers, out_ref = refs[:-1], refs[-1]
    stats = [own_ref[...]] + [r[...] for r in peers]
    weights = []
    for w in range(2):
        peaks = [s[w:w + 1] for s in stats]
        sums = [s[2 + w:3 + w] for s in stats]
        top = functools.reduce(jnp.maximum, peaks)
        total = sum(l * jnp.exp2(m - top) for m, l in zip(peaks, sums))
        weights.append(jnp.exp2(peaks[0] - top) / total)
    mixed = acc_ref[0] * weights[0] - acc_ref[1] * (weights[1] * lam_ref[row, 0])
    out_ref[...] = mixed.T.astype(jnp.bfloat16)


def mix(lam, acc, own, peers, row):
    _, dv, total = acc.shape
    B = 512
    return pl.pallas_call(
        functools.partial(mix_body, row=row),
        grid=(total // B,),
        out_shape=jax.ShapeDtypeStruct((total, dv), jnp.bfloat16),
        in_specs=[pl.BlockSpec(memory_space=pltpu.SMEM), pl.BlockSpec((2, dv, B), lambda i: (0, 0, i))]
        + [pl.BlockSpec((4, B), lambda i: (0, i))] * (1 + len(peers)),
        out_specs=pl.BlockSpec((B, dv), lambda i: (i, 0)),
        name="mix_wide" if dv == 256 else "mix_narrow",
        cost_estimate=pl.CostEstimate(flops=total * dv * 4, bytes_accessed=total * dv * 10, transcendentals=0),
    )(lam, acc, own, *peers)


def ring(axis, t):
    return lambda a: lax.ppermute(a, axis, [(i, (i + t) % 4) for i in range(4)])


SHIFTS = (0, 1, 3, 2)


def gather_parts(q, k, v):
    half = q.shape[0] // 2
    kv = jnp.concatenate([k, v], axis=1)
    swapped = lax.ppermute(kv[half:], "z", [(i, 3 - i) for i in range(4)])
    mine = jnp.concatenate([kv[:half], swapped], axis=0)
    kvs = [mine] + [ring("x", t)(mine) for t in SHIFTS[1:]]
    qs = [q] + [ring("z", t)(q) for t in SHIFTS[1:]]
    return qs, kvs


def positions():
    z, x = lax.axis_index("z"), lax.axis_index("x")
    return jnp.stack([jnp.int32(p) for p in positions_of(z, x)])


def positions_of(z, x, rows=768):
    half = rows // 2
    qp = [(4 * ((z + 4 - t) % 4) + x) * rows for t in SHIFTS]
    ns = [(x + 4 - t) % 4 for t in SHIFTS]
    return qp + [(4 * z + n) * rows for n in ns] + [(4 * (3 - z) + n) * rows + half for n in ns]


def combine(lam, acc, stat, row):
    rows = acc.shape[2] // 4
    peers = [ring("z", t)(stat_roll(stat, t)) for t in (1, 2, 3)]
    part = mix(lam, acc, stat, peers, row)
    slot = {t: i for i, t in enumerate(SHIFTS)}
    total = part[:rows].astype(jnp.float32)
    for t in (1, 3, 2):
        i = slot[t]
        back = lax.ppermute(part[i * rows:(i + 1) * rows], "z", [(j, (j - t) % 4) for j in range(4)])
        total = total + back.astype(jnp.float32)
    return (total * lax.rsqrt(jnp.mean(total * total, axis=-1, keepdims=True) + 1e-6)).astype(jnp.bfloat16)


def stat_roll(stat, t):
    rows = stat.shape[1] // 4
    slot = {s: i for i, s in enumerate(SHIFTS)}
    return jnp.concatenate([stat[:, slot[(s - t) % 4] * rows:(slot[(s - t) % 4] + 1) * rows] for s in SHIFTS], axis=1)


def attention(qw, kw, vw, qn, kn, vn, lam):
    qw, kw, vw, qn, kn, vn = (a[:, 0] for a in (qw, kw, vw, qn, kn, vn))
    pos = positions()
    qns, kvns = gather_parts(qn, kn, vn)
    qws, kvws = gather_parts(qw, kw, vw)
    accn, stn = flash(pos, qns, kvns, 64, 128)
    accw, stw = flash(pos, qws, kvws, 128, 256)
    heads_n = combine(lam, accn, stn, 1)
    heads_w = combine(lam, accw, stw, 0)
    return heads_w, heads_n


def cut_along(array, dim, peers):
    before, after = (array.shape[:dim], array.shape[dim + 1 :])
    return jnp.moveaxis(array.reshape(*before, peers, -1, *after), dim, 0)


def laid_out(pieces, dim):
    lengths = list(pieces.shape[1:])
    lengths[dim] *= pieces.shape[0]
    return jnp.moveaxis(pieces, 0, dim).reshape(lengths)


def moved_by_axis(pieces, axes, turns):
    inside = pieces.shape[1:]
    result = pieces.reshape(*(lax.axis_size(a) for a in axes), *inside)
    for k in turns:
        result = lax.all_to_all(result, axes[k], k, k, tiled=True)
    return result.reshape(-1, *inside)


def one_axis_at_a_time(array, axes, turns, split_dim, concat_dim):
    pieces = cut_along(array, split_dim, lax.axis_size(axes))
    return laid_out(moved_by_axis(pieces, axes, turns), concat_dim)


def exchange_in_groups(array, axis, split_dim, concat_dim, work, item_dim, out_dim):

    def moved(group):
        return lax.all_to_all(group, axis, split_axis=split_dim, concat_axis=concat_dim, tiled=True)

    items = jax.tree.leaves(array)[0].shape[item_dim]
    ends = [items * k // 2 for k in range(2 + 1)] if items % 2 == 0 else [0, items]
    groups = [
        jax.tree.map(lambda a: lax.slice_in_dim(a, low, high, axis=item_dim), array)
        for low, high in zip(ends, ends[1:])
    ]
    arrived = [moved(group) for group in groups]
    made = [work(group) for group in arrived]
    return jax.tree.map(lambda *parts: jnp.concatenate(parts, axis=out_dim), *made)


def shards(
    query_wide,
    key_wide,
    value_wide,
    query_narrow,
    key_narrow,
    value_narrow,
    mix_lambda,
    residual_in,
    out_wide,
    out_narrow,
    ffn_gain,
    expert_ids,
    expert_weights,
    gate_weight,
    up_weight,
    down_weight,
):
    tok_count, local_heads, _ = query_wide.shape
    heads_wide, heads_narrow = attention(
        query_wide, key_wide, value_wide, query_narrow, key_narrow, value_narrow, mix_lambda
    )
    tp_size = lax.axis_size(TP)
    local_rows = tok_count // tp_size
    whole_wide, whole_narrow = (
        lax.all_gather(out_wide, TP, axis=0, tiled=True),
        lax.all_gather(out_narrow, TP, axis=0, tiled=True),
    )
    mine_wide, mine_narrow = (
        one_axis_at_a_time(heads_wide, TP, (1, 0), 0, 1),
        one_axis_at_a_time(heads_narrow, TP, (1, 0), 0, 1),
    )
    projected = jnp.dot(mine_wide, whole_wide, preferred_element_type=jnp.float32) + jnp.dot(
        mine_narrow, whole_narrow, preferred_element_type=jnp.float32
    )
    stream = (projected + residual_in.astype(jnp.float32)).astype(jnp.bfloat16)
    stream_f = stream.astype(jnp.float32)
    normed = (
        stream_f
        * lax.rsqrt(jnp.mean(stream_f * stream_f, axis=-1, keepdims=True) + 1e-06)
        * ffn_gain
    ).astype(jnp.bfloat16)
    experts_all = lax.axis_size(SP) * tp_size
    capacity = max(2, 4 * local_rows // experts_all)
    model_width = normed.shape[1]
    flat_expert = expert_ids.reshape(-1)
    expert_hot = (flat_expert[:, None] == jnp.arange(experts_all, dtype=jnp.int32)[None, :]).astype(
        jnp.int32
    )
    slot_rank = jnp.sum((jnp.cumsum(expert_hot, axis=0) - 1) * expert_hot, axis=1)
    flat_slot = flat_expert * capacity + slot_rank
    slot_ids = jnp.arange(experts_all * capacity, dtype=jnp.int32)
    placed = slot_ids[:, None] == flat_slot[None, :]
    dispatch = jnp.any(placed.reshape(experts_all * capacity, local_rows, 2), axis=2).astype(
        jnp.bfloat16
    )
    outgoing = jnp.dot(dispatch, normed, preferred_element_type=jnp.float32).astype(jnp.bfloat16)
    outgoing = outgoing.reshape(experts_all, capacity, model_width)

    def serve_rows(arrived):
        sources, items, width = arrived.shape
        flat_rows = arrived.reshape(sources * items, width)
        gate_part = jnp.dot(flat_rows, gate_weight[0], preferred_element_type=jnp.float32)
        up_part = jnp.dot(flat_rows, up_weight[0], preferred_element_type=jnp.float32)
        hidden = (jax.nn.silu(gate_part) * up_part).astype(jnp.bfloat16)
        result = jnp.dot(hidden, down_weight[0], preferred_element_type=jnp.float32).astype(
            jnp.bfloat16
        )
        return lax.all_to_all(
            result.reshape(sources, items, width), SP_TP, split_axis=0, concat_axis=0, tiled=True
        )

    returned = exchange_in_groups(outgoing, SP_TP, 0, 0, serve_rows, 1, 1)
    slot_hot = (flat_slot[:, None] == slot_ids[None, :]).astype(
        jnp.float32
    ) * expert_weights.reshape(-1)[:, None]
    combine = jnp.sum(slot_hot.reshape(local_rows, 2, experts_all * capacity), axis=1)
    summed = jnp.dot(
        combine, returned.reshape(experts_all * capacity, model_width).astype(jnp.float32)
    )
    return (stream_f + summed).astype(jnp.bfloat16)


def solution(mesh):
    finer = Mesh(mesh.devices.reshape(4, 4, 4, 2), ("z", "x", "y", "c"))
    placed = (
        P(SP, TP, None),
        P(SP, TP, None),
        P(SP, TP, None),
        P(SP, TP, None),
        P(SP, TP, None),
        P(SP, TP, None),
        P(None, TP),
        P(SP_TP, None),
        P(TP, None),
        P(TP, None),
        P(),
        P(SP_TP, None),
        P(SP_TP, None),
        P(SP_TP, None, None),
        P(SP_TP, None, None),
        P(SP_TP, None, None),
    )
    return jax.shard_map(
        shards, mesh=finer, in_specs=placed, out_specs=P(SP_TP, None), check_vma=False
    )
```

```python
import functools
import jax
import jax.numpy as jnp
from jax import lax
from jax.experimental import pallas as pl
from jax.experimental.pallas import tpu as pltpu
from jax.sharding import Mesh
from jax.sharding import PartitionSpec as P

TP = ("y", "c")
SP = ("z", "x")
SP_TP = ("z", "x", "y", "c")

NEG = -1e30
LOG2E = 1.4426950408889634
TQ = 256
CH = 256
SHIFTS = (0, 1, 3, 2)
SLOT = {t: i for i, t in enumerate(SHIFTS)}


class Copies:
    def __init__(self, send_sems, recv_sems):
        self.send_sems, self.recv_sems, self.all = send_sems, recv_sems, []

    def make(self, src, dst, **device):
        n = len(self.all)
        copy = pltpu.make_async_remote_copy(
            src_ref=src,
            dst_ref=dst,
            send_sem=self.send_sems.at[n],
            recv_sem=self.recv_sems.at[n],
            device_id=device,
            device_id_type=pl.DeviceIdType.MESH,
        )
        self.all.append(copy)
        return copy


class Heads:
    def __init__(self, d, dv, rows, ins, refs, shared, copies):
        self.d, self.dv, self.rows, self.half = d, dv, rows, rows // 2
        self.q_in, self.kv_in = ins
        self.q_s, self.kv_s, self.qt_s, self.vt_s, self.acc, self.st, self.st_in, self.part, self.part_in, self.relay, self.heads, self.out = refs
        self.tab, self.pos, self.s_a, self.s_b, self.t_a, self.t_b, self.p_scr, self.m_s, self.l_s = shared
        self.scale = d ** (-0.5) * LOG2E
        self.copies = copies
        z, x = lax.axis_index("z"), lax.axis_index("x")
        up = {"z": (z + 1) % 4}, {"z": (z + 3) % 4}
        right = {"x": (x + 1) % 4}, {"x": (x + 3) % 4}
        half = self.half
        one, three, two = SLOT[1], SLOT[3], SLOT[2]
        h0, h1 = pl.ds(0, half), pl.ds(half, half)
        self.q_near = [copies.make(self.q_in, self.q_s.at[one], **up[0]), copies.make(self.q_in, self.q_s.at[three], **up[1])]
        self.q_far = [
            copies.make(self.q_s.at[one, h0], self.q_s.at[two, h0], **up[0]),
            copies.make(self.q_s.at[three, h1], self.q_s.at[two, h1], **up[1]),
        ]
        self.swap = copies.make(self.kv_in.at[h1], self.kv_s.at[1, 0], z=3 - z)
        self.kv_near, self.kv_far = [], []
        quarter = half // 2
        g0, g1 = pl.ds(0, quarter), pl.ds(quarter, quarter)
        for b in range(2):
            src = self.kv_in.at[h0] if b == 0 else self.kv_s.at[1, 0]
            self.kv_near.append([copies.make(src, self.kv_s.at[b, one], **right[0]), copies.make(src, self.kv_s.at[b, three], **right[1])])
            self.kv_far.append([
                copies.make(self.kv_s.at[b, one, g0], self.kv_s.at[b, two, g0], **right[0]),
                copies.make(self.kv_s.at[b, three, g1], self.kv_s.at[b, two, g1], **right[1]),
            ])
        self.st_out = [copies.make(self.st, self.st_in.at[t - 1], z=(z + t) % 4) for t in (1, 2, 3)]
        self.part_near = [
            copies.make(self.part.at[one], self.part_in.at[0], **up[1]),
            copies.make(self.part.at[three], self.part_in.at[1], **up[0]),
        ]
        self.part_first = [
            copies.make(self.part.at[two, h0], self.relay.at[0], **up[0]),
            copies.make(self.part.at[two, h1], self.relay.at[1], **up[1]),
        ]
        self.part_far = [
            copies.make(self.relay.at[0], self.part_in.at[2, h0], **up[0]),
            copies.make(self.relay.at[1], self.part_in.at[2, h1], **up[1]),
        ]
        rank = lax.axis_index("y") * 2 + lax.axis_index("c")
        self.rank = rank
        mine = rows // 8
        self.to_tokens = []
        for k in range(1, 8):
            r = (rank + k) % 8
            self.to_tokens.append(copies.make(
                self.heads.at[pl.ds(pl.multiple_of(r * mine, mine), mine)],
                self.out.at[:, pl.ds(pl.multiple_of(rank * dv, dv), dv)],
                y=r // 2, c=r % 2,
            ))

    def send_swap(self):
        self.swap.start()

    def send_near(self):
        for c in self.kv_near[0] + self.q_near:
            c.start()

    def pass_swap(self):
        self.swap.wait_recv()
        for c in self.kv_near[1]:
            c.start()

    def relay_first(self):
        for near, far in zip(self.kv_near[0] + self.q_near, self.kv_far[0] + self.q_far):
            near.wait_recv()
            far.start()

    def relay_second(self):
        for near, far in zip(self.kv_near[1], self.kv_far[1]):
            near.wait_recv()
            far.start()

    def wait_all(self):
        for c in self.kv_far[0] + self.kv_far[1] + self.q_far:
            c.wait_recv()

    def prepare(self):
        d, dv, rows, half = self.d, self.dv, self.rows, self.half

        def turn(i, _):
            r = pl.multiple_of(i * rows, rows)
            self.qt_s[:, pl.ds(r, rows)] = self.q_s[i].T
            return 0
        lax.fori_loop(0, 4, turn, 0)

        def turn_v(i, _):
            r = pl.multiple_of(i * half, half)
            self.vt_s[:, pl.ds(r, half)] = self.kv_s[i // 4, i % 4, :, 2 * d:2 * d + dv].T
            return 0
        lax.fori_loop(0, 8, turn_v, 0)

    def read(self, i, s_buf, t_buf):
        d, half = self.d, self.half
        q0 = pl.multiple_of(self.tab[0, i] * TQ, TQ)
        kj = self.tab[1, i]
        part, first = kj // 2, (kj % 2) * 2
        for w in range(2):
            qt = self.qt_s[w * d:(w + 1) * d, pl.ds(q0, TQ)]
            top = None
            for c in range(2):
                k = self.kv_s[part, first + c, :, w * d:(w + 1) * d]
                s = jnp.dot(k, qt, preferred_element_type=jnp.float32)
                s_buf[w, c * half:(c + 1) * half] = s
                m8 = jnp.max(s.reshape(half // 8, 8, TQ), axis=0)
                top = m8 if top is None else jnp.maximum(top, m8)
            t_buf[w] = top

    def mask(self, i, s_buf, t_buf):
        rows, half = self.rows, self.half
        per = rows // TQ
        qi, kj = self.tab[0, i], self.tab[1, i]
        qp = self.pos[qi // per] + (qi % per) * TQ
        CM = 128
        t_buf[...] = jnp.full_like(t_buf, NEG)

        def chunk(c, _):
            r = pl.multiple_of(c * CM, CM)
            late = c // (half // CM)
            k0 = self.pos[4 + 2 * kj + late] + (c - late * (half // CM)) * CM
            keep = lax.broadcasted_iota(jnp.int32, (CM, TQ), 0) - lax.broadcasted_iota(jnp.int32, (CM, TQ), 1) <= qp - k0
            for w in range(2):
                s = jnp.where(keep, s_buf[w, pl.ds(r, CM)], NEG)
                s_buf[w, pl.ds(r, CM)] = s
                t_buf[w] = jnp.maximum(t_buf[w], jnp.max(s.reshape(CM // 8, 8, TQ), axis=0))
            return 0
        lax.fori_loop(0, rows // CM, chunk, 0)

    def weigh(self, i, q0, s_buf, t_buf):
        rows = self.rows
        k0 = pl.multiple_of(self.tab[1, i] * rows, rows)
        for w in range(2):
            old = self.m_s[w:w + 1]
            new = jnp.maximum(old, jnp.max(t_buf[w], axis=0, keepdims=True) * self.scale)
            f = jnp.exp2(old - new)
            self.m_s[w:w + 1] = new
            tot = None
            for c in range(rows // CH):
                p = jnp.exp2(s_buf[w, c * CH:(c + 1) * CH] * self.scale - new)
                t8 = jnp.sum(p.reshape(CH // 8, 8, TQ), axis=0)
                tot = t8 if tot is None else tot + t8
                self.p_scr[w, c * CH:(c + 1) * CH] = p.astype(jnp.bfloat16)
            o = jnp.dot(self.vt_s[:, pl.ds(k0, rows)], self.p_scr[w], preferred_element_type=jnp.float32)
            self.l_s[w] = self.l_s[w] * f + tot
            self.acc[w, :, pl.ds(q0, TQ)] = self.acc[w, :, pl.ds(q0, TQ)] * f + o

    def run(self, steps, hooks):
        def advance(i, cur, nxt):
            q0 = pl.multiple_of(self.tab[0, i] * TQ, TQ)

            @pl.when(self.tab[3, i] == 1)
            def _():
                self.m_s[...] = jnp.full_like(self.m_s, NEG)
                self.l_s[...] = jnp.zeros_like(self.l_s)
                self.acc[:, :, pl.ds(q0, TQ)] = jnp.zeros((2, self.dv, TQ), jnp.float32)

            @pl.when(self.tab[2, i] == 1)
            def _():
                self.mask(i, *cur)
            self.read(jnp.minimum(i + 1, steps - 1), *nxt)
            self.weigh(i, q0, *cur)

            @pl.when(self.tab[3, i + 1] == 1)
            def _():
                self.st[0:2, pl.ds(q0, TQ)] = self.m_s[...]
                for w in range(2):
                    self.st[2 + w:3 + w, pl.ds(q0, TQ)] = jnp.sum(self.l_s[w], axis=0, keepdims=True)

        one, two = (self.s_a, self.t_a), (self.s_b, self.t_b)
        self.read(0, *one)
        pairs = (steps + 1) // 2

        def pair(n, _):
            for k, hook in enumerate(hooks):
                pl.when(n == pairs * (k + 1) // (len(hooks) + 1))(hook)
            advance(2 * n, one, two)

            @pl.when(2 * n + 1 < steps)
            def _():
                advance(2 * n + 1, two, one)
            return 0
        lax.fori_loop(0, pairs, pair, 0)

    def mix(self, slot, lam):
        rows, dv = self.rows, self.dv
        for p in range(rows // TQ):
            c0 = slot * rows + p * TQ
            stats = [self.st[:, c0:c0 + TQ]]
            for t in (1, 2, 3):
                at = SLOT[(SHIFTS[slot] - t) % 4] * rows + p * TQ
                stats.append(self.st_in[t - 1, :, at:at + TQ])
            weights = []
            for w in range(2):
                peaks = [s[w:w + 1] for s in stats]
                top = functools.reduce(jnp.maximum, peaks)
                total = sum(s[2 + w:3 + w] * jnp.exp2(m - top) for m, s in zip(peaks, stats))
                weights.append(jnp.exp2(peaks[0] - top) / total)
            mixed = self.acc[0, :, c0:c0 + TQ] * weights[0] - self.acc[1, :, c0:c0 + TQ] * (weights[1] * lam)
            self.part[slot, p * TQ:(p + 1) * TQ] = mixed.T.astype(jnp.bfloat16)

    def send_stats(self):
        for c in self.st_out:
            c.start()

    def mix_and_send(self, lam):
        for c in self.st_out:
            c.wait_recv()
        self.mix(SLOT[2], lam)
        for c in self.part_first:
            c.start()
        self.mix(SLOT[1], lam)
        self.part_near[0].start()
        self.mix(SLOT[3], lam)
        self.part_near[1].start()

    def pass_parts(self):
        for first, far in zip(self.part_first, self.part_far):
            first.wait_recv()
            far.start()

    def finish(self):
        for c in self.part_near + self.part_far:
            c.wait_recv()
        B = 192
        for p in range(self.rows // B):
            r = slice(p * B, (p + 1) * B)
            total = self.part[0, r].astype(jnp.float32)
            for n in range(3):
                total = total + self.part_in[n, r].astype(jnp.float32)
            total = total * lax.rsqrt(jnp.mean(total * total, axis=-1, keepdims=True) + 1e-06)
            self.heads[r] = total.astype(jnp.bfloat16)
        for c in self.to_tokens:
            c.start()
        mine = self.rows // 8
        at = pl.multiple_of(self.rank * mine, mine)
        self.out[:, pl.ds(pl.multiple_of(self.rank * self.dv, self.dv), self.dv)] = self.heads[pl.ds(at, mine)]


def attention_kernel(lam_ref, qn_in, kvn_in, qw_in, kvw_in, out_w, out_n, *scratch, rows):
    narrow_refs, wide_refs = scratch[:12], scratch[12:24]
    shared, (send_sems, recv_sems, local_sems) = scratch[24:33], scratch[33:36]
    z, x = lax.axis_index("z"), lax.axis_index("x")
    half = rows // 2
    copies = Copies(send_sems, recv_sems)
    narrow = Heads(64, 128, rows, (qn_in, kvn_in), narrow_refs, shared, copies)
    wide = Heads(128, 256, rows, (qw_in, kvw_in), wide_refs, shared, copies)

    barrier = pltpu.get_barrier_semaphore()
    for t in (1, 2, 3):
        pl.semaphore_signal(barrier, inc=1, device_id={"z": (z + t) % 4}, device_id_type=pl.DeviceIdType.MESH)
        pl.semaphore_signal(barrier, inc=1, device_id={"x": (x + t) % 4}, device_id_type=pl.DeviceIdType.MESH)
    rank = narrow.rank
    for k in range(1, 8):
        r = (rank + k) % 8
        pl.semaphore_signal(barrier, inc=1, device_id={"y": r // 2, "c": r % 2}, device_id_type=pl.DeviceIdType.MESH)
    local = []
    for h in (narrow, wide):
        local.append(pltpu.make_async_copy(h.q_in, h.q_s.at[0], local_sems.at[len(local)]))
        local.append(pltpu.make_async_copy(h.kv_in.at[pl.ds(0, half)], h.kv_s.at[0, 0], local_sems.at[len(local)]))
    for c in local:
        c.start()
    pl.semaphore_wait(barrier, 13)

    narrow.send_swap()
    narrow.send_near()
    wide.send_swap()
    narrow.pass_swap()
    wide.send_near()

    pos, tab = narrow.pos, narrow.tab
    for i, t in enumerate(SHIFTS):
        pos[i] = (4 * ((z + 4 - t) % 4) + x) * rows
        n = (x + 4 - t) % 4
        pos[4 + i] = (4 * z + n) * rows
        pos[8 + i] = (4 * (3 - z) + n) * rows + half
    per = rows // TQ

    def list_q(qi, n):
        qp = pos[qi // per] + (qi % per) * TQ

        def list_k(kj, carry):
            n, first = carry
            p0, p1 = pos[4 + 2 * kj], pos[4 + 2 * kj + 1]
            hi, lo = jnp.maximum(p0, p1), jnp.minimum(p0, p1)
            full = hi + half - 1 <= qp
            some = lo <= qp + TQ - 1
            tab[0, n] = qi
            tab[1, n] = kj
            tab[2, n] = jnp.where(full, 0, 1)
            tab[3, n] = first
            return n + jnp.where(some, 1, 0), jnp.where(some, 0, first)
        m, _ = lax.fori_loop(0, 4, list_k, (n, 1))

        @pl.when(m == n)
        def _():
            tab[0, n] = qi
            tab[1, n] = 0
            tab[2, n] = 1
            tab[3, n] = 1
        return jnp.maximum(m, n + 1)
    steps = lax.fori_loop(0, 4 * per, list_q, 0)
    tab[3, steps] = 1

    narrow.relay_first()
    narrow.relay_second()
    wide.pass_swap()
    narrow.wait_all()
    for c in local:
        c.wait()
    narrow.prepare()
    narrow.run(steps, [wide.relay_first, wide.relay_second])
    narrow.send_stats()
    wide.wait_all()
    wide.prepare()
    narrow.mix_and_send(lam_ref[1, 0])
    narrow.mix(0, lam_ref[1, 0])
    wide.run(steps, [narrow.pass_parts, narrow.finish])
    wide.send_stats()
    wide.mix_and_send(lam_ref[0, 0])
    wide.pass_parts()
    wide.mix(0, lam_ref[0, 0])
    wide.finish()
    for h in (narrow, wide):
        for c in h.to_tokens:
            c.wait_recv()
    out_n[...] = narrow.out[...]
    out_w[...] = wide.out[...]
    for c in copies.all:
        c.wait_send()


def attention(qw, kw, vw, qn, kn, vn, lam):
    qw, kw, vw, qn, kn, vn = (a[:, 0] for a in (qw, kw, vw, qn, kn, vn))
    rows = qw.shape[0]
    half, mine = rows // 2, rows // 8

    def scratch(d, dv):
        return [
            pltpu.VMEM((4, rows, 2 * d), jnp.bfloat16),
            pltpu.VMEM((2, 4, half, 2 * d + dv), jnp.bfloat16),
            pltpu.VMEM((2 * d, 4 * rows), jnp.bfloat16),
            pltpu.VMEM((dv, 4 * rows), jnp.bfloat16),
            pltpu.VMEM((2, dv, 4 * rows), jnp.float32),
            pltpu.VMEM((4, 4 * rows), jnp.float32),
            pltpu.VMEM((3, 4, 4 * rows), jnp.float32),
            pltpu.VMEM((4, rows, dv), jnp.bfloat16),
            pltpu.VMEM((3, rows, dv), jnp.bfloat16),
            pltpu.VMEM((2, half, dv), jnp.bfloat16),
            pltpu.VMEM((rows, dv), jnp.bfloat16),
            pltpu.VMEM((mine, 8 * dv), jnp.bfloat16),
        ]
    any_ = pl.BlockSpec(memory_space=pl.ANY)
    vmem = pl.BlockSpec(memory_space=pltpu.VMEM)
    count = 2 * (2 + 2 + 1 + 8 + 3 + 6 + 7)
    return pl.pallas_call(
        functools.partial(attention_kernel, rows=rows),
        out_shape=(jax.ShapeDtypeStruct((mine, 8 * 256), jnp.bfloat16), jax.ShapeDtypeStruct((mine, 8 * 128), jnp.bfloat16)),
        in_specs=[pl.BlockSpec(memory_space=pltpu.SMEM)] + [any_] * 4,
        out_specs=(vmem, vmem),
        scratch_shapes=scratch(64, 128) + scratch(128, 256) + [
            pltpu.SMEM((4, 4 * (rows // TQ) * 4 + 1), jnp.int32),
            pltpu.SMEM((12,), jnp.int32),
            pltpu.VMEM((2, rows, TQ), jnp.float32),
            pltpu.VMEM((2, rows, TQ), jnp.float32),
            pltpu.VMEM((2, 8, TQ), jnp.float32),
            pltpu.VMEM((2, 8, TQ), jnp.float32),
            pltpu.VMEM((2, rows, TQ), jnp.bfloat16),
            pltpu.VMEM((2, TQ), jnp.float32),
            pltpu.VMEM((2, 8, TQ), jnp.float32),
            pltpu.SemaphoreType.DMA((count,)),
            pltpu.SemaphoreType.DMA((count,)),
            pltpu.SemaphoreType.DMA((4,)),
        ],
        name="attention",
        cost_estimate=pl.CostEstimate(flops=100 * 10**9, bytes_accessed=10**7, transcendentals=0),
        compiler_params=pltpu.CompilerParams(collective_id=0, has_side_effects=True, vmem_limit_bytes=60 * 2**20),
    )(lam, qn, jnp.concatenate([kn, vn], axis=1), qw, jnp.concatenate([kw, vw], axis=1))


def exchange_in_groups(array, axis, split_dim, concat_dim, work, item_dim, out_dim):

    def moved(group):
        return lax.all_to_all(group, axis, split_axis=split_dim, concat_axis=concat_dim, tiled=True)

    items = jax.tree.leaves(array)[0].shape[item_dim]
    ends = [items * k // 2 for k in range(2 + 1)] if items % 2 == 0 else [0, items]
    groups = [
        jax.tree.map(lambda a: lax.slice_in_dim(a, low, high, axis=item_dim), array)
        for low, high in zip(ends, ends[1:])
    ]
    arrived = [moved(group) for group in groups]
    made = [work(group) for group in arrived]
    return jax.tree.map(lambda *parts: jnp.concatenate(parts, axis=out_dim), *made)


def shards(
    query_wide,
    key_wide,
    value_wide,
    query_narrow,
    key_narrow,
    value_narrow,
    mix_lambda,
    residual_in,
    out_wide,
    out_narrow,
    ffn_gain,
    expert_ids,
    expert_weights,
    gate_weight,
    up_weight,
    down_weight,
):
    tok_count, local_heads, _ = query_wide.shape
    mine_wide, mine_narrow = attention(
        query_wide, key_wide, value_wide, query_narrow, key_narrow, value_narrow, mix_lambda
    )
    tp_size = lax.axis_size(TP)
    local_rows = tok_count // tp_size
    whole_wide, whole_narrow = (
        lax.all_gather(out_wide, TP, axis=0, tiled=True),
        lax.all_gather(out_narrow, TP, axis=0, tiled=True),
    )
    projected = jnp.dot(mine_wide, whole_wide, preferred_element_type=jnp.float32) + jnp.dot(
        mine_narrow, whole_narrow, preferred_element_type=jnp.float32
    )
    stream = (projected + residual_in.astype(jnp.float32)).astype(jnp.bfloat16)
    stream_f = stream.astype(jnp.float32)
    normed = (
        stream_f
        * lax.rsqrt(jnp.mean(stream_f * stream_f, axis=-1, keepdims=True) + 1e-06)
        * ffn_gain
    ).astype(jnp.bfloat16)
    experts_all = lax.axis_size(SP) * tp_size
    capacity = max(2, 4 * local_rows // experts_all)
    model_width = normed.shape[1]
    flat_expert = expert_ids.reshape(-1)
    expert_hot = (flat_expert[:, None] == jnp.arange(experts_all, dtype=jnp.int32)[None, :]).astype(
        jnp.int32
    )
    slot_rank = jnp.sum((jnp.cumsum(expert_hot, axis=0) - 1) * expert_hot, axis=1)
    flat_slot = flat_expert * capacity + slot_rank
    slot_ids = jnp.arange(experts_all * capacity, dtype=jnp.int32)
    placed = slot_ids[:, None] == flat_slot[None, :]
    dispatch = jnp.any(placed.reshape(experts_all * capacity, local_rows, 2), axis=2).astype(
        jnp.bfloat16
    )
    outgoing = jnp.dot(dispatch, normed, preferred_element_type=jnp.float32).astype(jnp.bfloat16)
    outgoing = outgoing.reshape(experts_all, capacity, model_width)

    def serve_rows(arrived):
        sources, items, width = arrived.shape
        flat_rows = arrived.reshape(sources * items, width)
        gate_part = jnp.dot(flat_rows, gate_weight[0], preferred_element_type=jnp.float32)
        up_part = jnp.dot(flat_rows, up_weight[0], preferred_element_type=jnp.float32)
        hidden = (jax.nn.silu(gate_part) * up_part).astype(jnp.bfloat16)
        result = jnp.dot(hidden, down_weight[0], preferred_element_type=jnp.float32).astype(
            jnp.bfloat16
        )
        return lax.all_to_all(
            result.reshape(sources, items, width), SP_TP, split_axis=0, concat_axis=0, tiled=True
        )

    returned = exchange_in_groups(outgoing, SP_TP, 0, 0, serve_rows, 1, 1)
    slot_hot = (flat_slot[:, None] == slot_ids[None, :]).astype(
        jnp.float32
    ) * expert_weights.reshape(-1)[:, None]
    combine = jnp.sum(slot_hot.reshape(local_rows, 2, experts_all * capacity), axis=1)
    summed = jnp.dot(
        combine, returned.reshape(experts_all * capacity, model_width).astype(jnp.float32)
    )
    return (stream_f + summed).astype(jnp.bfloat16)


def solution(mesh):
    finer = Mesh(mesh.devices.reshape(4, 4, 4, 2), ("z", "x", "y", "c"))
    placed = (
        P(SP, TP, None),
        P(SP, TP, None),
        P(SP, TP, None),
        P(SP, TP, None),
        P(SP, TP, None),
        P(SP, TP, None),
        P(None, TP),
        P(SP_TP, None),
        P(TP, None),
        P(TP, None),
        P(),
        P(SP_TP, None),
        P(SP_TP, None),
        P(SP_TP, None, None),
        P(SP_TP, None, None),
        P(SP_TP, None, None),
    )
    return jax.shard_map(
        shards, mesh=finer, in_specs=placed, out_specs=P(SP_TP, None), check_vma=False
    )
```

```python
import functools
import jax
import jax.numpy as jnp
from jax import lax
from jax.experimental import pallas as pl
from jax.experimental.pallas import tpu as pltpu
from jax.sharding import Mesh
from jax.sharding import PartitionSpec as P

TP = ("y", "c")
SP = ("z", "x")
SP_TP = ("z", "x", "y", "c")

NEG = -1e30
LOG2E = 1.4426950408889634
TQ = 256
CH = 256
SHIFTS = (0, 1, 3, 2)
SLOT = {t: i for i, t in enumerate(SHIFTS)}


class Copies:
    def __init__(self, send_sems, recv_sems):
        self.send_sems, self.recv_sems, self.all = send_sems, recv_sems, []

    def make(self, src, dst, **device):
        n = len(self.all)
        copy = pltpu.make_async_remote_copy(
            src_ref=src,
            dst_ref=dst,
            send_sem=self.send_sems.at[n],
            recv_sem=self.recv_sems.at[n],
            device_id=device,
            device_id_type=pl.DeviceIdType.MESH,
        )
        self.all.append(copy)
        return copy


class Heads:
    def __init__(self, d, dv, rows, ins, refs, shared, copies):
        self.d, self.dv, self.rows, self.half = d, dv, rows, rows // 2
        self.q_in, self.kv_in = ins
        self.q_s, self.kv_s, self.qt_s, self.vt_s, self.acc, self.st, self.st_in, self.part, self.part_in, self.relay, self.heads, self.out = refs
        self.tab, self.pos, self.s_a, self.s_b, self.t_a, self.t_b, self.p_scr, self.m_s, self.l_s = shared
        self.scale = d ** (-0.5) * LOG2E
        self.copies = copies
        z, x = lax.axis_index("z"), lax.axis_index("x")
        up = {"z": (z + 1) % 4}, {"z": (z + 3) % 4}
        right = {"x": (x + 1) % 4}, {"x": (x + 3) % 4}
        half = self.half
        one, three, two = SLOT[1], SLOT[3], SLOT[2]
        h0, h1 = pl.ds(0, half), pl.ds(half, half)
        self.q_near = [copies.make(self.q_in, self.q_s.at[one], **up[0]), copies.make(self.q_in, self.q_s.at[three], **up[1])]
        self.q_far = [
            copies.make(self.q_s.at[one, h0], self.q_s.at[two, h0], **up[0]),
            copies.make(self.q_s.at[three, h1], self.q_s.at[two, h1], **up[1]),
        ]
        self.swap = copies.make(self.kv_in.at[h1], self.kv_s.at[1, 0], z=3 - z)
        self.kv_near, self.kv_far = [], []
        quarter = half // 2
        g0, g1 = pl.ds(0, quarter), pl.ds(quarter, quarter)
        for b in range(2):
            src = self.kv_in.at[h0] if b == 0 else self.kv_s.at[1, 0]
            self.kv_near.append([copies.make(src, self.kv_s.at[b, one], **right[0]), copies.make(src, self.kv_s.at[b, three], **right[1])])
            self.kv_far.append([
                copies.make(self.kv_s.at[b, one, g0], self.kv_s.at[b, two, g0], **right[0]),
                copies.make(self.kv_s.at[b, three, g1], self.kv_s.at[b, two, g1], **right[1]),
            ])
        self.st_out = [copies.make(self.st, self.st_in.at[t - 1], z=(z + t) % 4) for t in (1, 2, 3)]
        self.part_near = [
            copies.make(self.part.at[one], self.part_in.at[0], **up[1]),
            copies.make(self.part.at[three], self.part_in.at[1], **up[0]),
        ]
        self.part_first = [
            copies.make(self.part.at[two, h0], self.relay.at[0], **up[0]),
            copies.make(self.part.at[two, h1], self.relay.at[1], **up[1]),
        ]
        self.part_far = [
            copies.make(self.relay.at[0], self.part_in.at[2, h0], **up[0]),
            copies.make(self.relay.at[1], self.part_in.at[2, h1], **up[1]),
        ]
        rank = lax.axis_index("y") * 2 + lax.axis_index("c")
        self.rank = rank
        mine = rows // 8
        self.to_tokens = []
        for k in range(1, 8):
            r = (rank + k) % 8
            self.to_tokens.append(copies.make(
                self.heads.at[pl.ds(pl.multiple_of(r * mine, mine), mine)],
                self.out.at[:, pl.ds(pl.multiple_of(rank * dv, dv), dv)],
                y=r // 2, c=r % 2,
            ))

    def send_swap(self):
        self.swap.start()

    def send_near(self):
        for c in self.kv_near[0] + self.q_near:
            c.start()

    def pass_swap(self):
        self.swap.wait_recv()
        for c in self.kv_near[1]:
            c.start()

    def relay_first(self):
        for near, far in zip(self.kv_near[0] + self.q_near, self.kv_far[0] + self.q_far):
            near.wait_recv()
            far.start()

    def relay_second(self):
        for near, far in zip(self.kv_near[1], self.kv_far[1]):
            near.wait_recv()
            far.start()

    def wait_all(self):
        for c in self.kv_far[0] + self.kv_far[1] + self.q_far:
            c.wait_recv()

    def prepare(self):
        d, dv, rows, half = self.d, self.dv, self.rows, self.half

        def turn(i, _):
            r = pl.multiple_of(i * rows, rows)
            self.qt_s[:, pl.ds(r, rows)] = self.q_s[i].T
            return 0
        lax.fori_loop(0, 4, turn, 0)

        def turn_v(i, _):
            r = pl.multiple_of(i * half, half)
            self.vt_s[:, pl.ds(r, half)] = self.kv_s[i // 4, i % 4, :, 2 * d:2 * d + dv].T
            return 0
        lax.fori_loop(0, 8, turn_v, 0)

    def read(self, i, s_buf, t_buf):
        d, half = self.d, self.half
        q0 = pl.multiple_of(self.tab[0, i] * TQ, TQ)
        kj = self.tab[1, i]
        part, first = kj // 2, (kj % 2) * 2
        for w in range(2):
            qt = self.qt_s[w * d:(w + 1) * d, pl.ds(q0, TQ)]
            top = None
            for c in range(2):
                k = self.kv_s[part, first + c, :, w * d:(w + 1) * d]
                s = jnp.dot(k, qt, preferred_element_type=jnp.float32)
                s_buf[w, c * half:(c + 1) * half] = s
                m8 = jnp.max(s.reshape(half // 8, 8, TQ), axis=0)
                top = m8 if top is None else jnp.maximum(top, m8)
            t_buf[w] = top

    def mask(self, i, s_buf, t_buf):
        rows, half = self.rows, self.half
        per = rows // TQ
        qi, kj = self.tab[0, i], self.tab[1, i]
        qp = self.pos[qi // per] + (qi % per) * TQ
        CM = 128
        t_buf[...] = jnp.full_like(t_buf, NEG)

        def chunk(c, _):
            r = pl.multiple_of(c * CM, CM)
            late = c // (half // CM)
            k0 = self.pos[4 + 2 * kj + late] + (c - late * (half // CM)) * CM
            keep = lax.broadcasted_iota(jnp.int32, (CM, TQ), 0) - lax.broadcasted_iota(jnp.int32, (CM, TQ), 1) <= qp - k0
            for w in range(2):
                s = jnp.where(keep, s_buf[w, pl.ds(r, CM)], NEG)
                s_buf[w, pl.ds(r, CM)] = s
                t_buf[w] = jnp.maximum(t_buf[w], jnp.max(s.reshape(CM // 8, 8, TQ), axis=0))
            return 0
        lax.fori_loop(0, rows // CM, chunk, 0)

    def weigh(self, i, q0, s_buf, t_buf):
        rows = self.rows
        k0 = pl.multiple_of(self.tab[1, i] * rows, rows)
        for w in range(2):
            old = self.m_s[w:w + 1]
            new = jnp.maximum(old, jnp.max(t_buf[w], axis=0, keepdims=True) * self.scale)
            f = jnp.exp2(old - new)
            self.m_s[w:w + 1] = new
            tot = None
            for c in range(rows // CH):
                p = jnp.exp2(s_buf[w, c * CH:(c + 1) * CH] * self.scale - new)
                t8 = jnp.sum(p.reshape(CH // 8, 8, TQ), axis=0)
                tot = t8 if tot is None else tot + t8
                self.p_scr[w, c * CH:(c + 1) * CH] = p.astype(jnp.bfloat16)
            o = jnp.dot(self.vt_s[:, pl.ds(k0, rows)], self.p_scr[w], preferred_element_type=jnp.float32)
            self.l_s[w] = self.l_s[w] * f + tot
            self.acc[w, :, pl.ds(q0, TQ)] = self.acc[w, :, pl.ds(q0, TQ)] * f + o

    def run(self, steps, hooks):
        def advance(i, cur, nxt):
            q0 = pl.multiple_of(self.tab[0, i] * TQ, TQ)

            @pl.when(self.tab[3, i] == 1)
            def _():
                self.m_s[...] = jnp.full_like(self.m_s, NEG)
                self.l_s[...] = jnp.zeros_like(self.l_s)
                self.acc[:, :, pl.ds(q0, TQ)] = jnp.zeros((2, self.dv, TQ), jnp.float32)

            @pl.when(self.tab[2, i] == 1)
            def _():
                self.mask(i, *cur)
            self.read(jnp.minimum(i + 1, steps - 1), *nxt)
            self.weigh(i, q0, *cur)

            @pl.when(self.tab[3, i + 1] == 1)
            def _():
                self.st[0:2, pl.ds(q0, TQ)] = self.m_s[...]
                for w in range(2):
                    self.st[2 + w:3 + w, pl.ds(q0, TQ)] = jnp.sum(self.l_s[w], axis=0, keepdims=True)

        one, two = (self.s_a, self.t_a), (self.s_b, self.t_b)
        self.read(0, *one)
        pairs = (steps + 1) // 2

        def pair(n, _):
            for k, hook in enumerate(hooks):
                pl.when(n == pairs * (k + 1) // (len(hooks) + 1))(hook)
            advance(2 * n, one, two)

            @pl.when(2 * n + 1 < steps)
            def _():
                advance(2 * n + 1, two, one)
            return 0
        lax.fori_loop(0, pairs, pair, 0)

    def mix(self, slot, lam):
        rows, dv = self.rows, self.dv
        for p in range(rows // TQ):
            c0 = slot * rows + p * TQ
            stats = [self.st[:, c0:c0 + TQ]]
            for t in (1, 2, 3):
                at = SLOT[(SHIFTS[slot] - t) % 4] * rows + p * TQ
                stats.append(self.st_in[t - 1, :, at:at + TQ])
            weights = []
            for w in range(2):
                peaks = [s[w:w + 1] for s in stats]
                top = functools.reduce(jnp.maximum, peaks)
                total = sum(s[2 + w:3 + w] * jnp.exp2(m - top) for m, s in zip(peaks, stats))
                weights.append(jnp.exp2(peaks[0] - top) / total)
            mixed = self.acc[0, :, c0:c0 + TQ] * weights[0] - self.acc[1, :, c0:c0 + TQ] * (weights[1] * lam)
            self.part[slot, p * TQ:(p + 1) * TQ] = mixed.T.astype(jnp.bfloat16)

    def send_stats(self):
        for c in self.st_out:
            c.start()

    def mix_and_send(self, lam):
        for c in self.st_out:
            c.wait_recv()
        self.mix(SLOT[2], lam)
        for c in self.part_first:
            c.start()
        self.mix(SLOT[1], lam)
        self.part_near[0].start()
        self.mix(SLOT[3], lam)
        self.part_near[1].start()

    def pass_parts(self):
        for first, far in zip(self.part_first, self.part_far):
            first.wait_recv()
            far.start()

    def finish(self):
        for c in self.part_near + self.part_far:
            c.wait_recv()
        B = 192
        for p in range(self.rows // B):
            r = slice(p * B, (p + 1) * B)
            total = self.part[0, r].astype(jnp.float32)
            for n in range(3):
                total = total + self.part_in[n, r].astype(jnp.float32)
            total = total * lax.rsqrt(jnp.mean(total * total, axis=-1, keepdims=True) + 1e-06)
            self.heads[r] = total.astype(jnp.bfloat16)
        for c in self.to_tokens:
            c.start()
        mine = self.rows // 8
        at = pl.multiple_of(self.rank * mine, mine)
        self.out[:, pl.ds(pl.multiple_of(self.rank * self.dv, self.dv), self.dv)] = self.heads[pl.ds(at, mine)]


def attention_kernel(lam_ref, qn_in, kvn_in, qw_in, kvw_in, out_w, out_n, *scratch, rows):
    narrow_refs, wide_refs = scratch[:12], scratch[12:24]
    shared, (send_sems, recv_sems, local_sems) = scratch[24:33], scratch[33:36]
    z, x = lax.axis_index("z"), lax.axis_index("x")
    half = rows // 2
    copies = Copies(send_sems, recv_sems)
    narrow = Heads(64, 128, rows, (qn_in, kvn_in), narrow_refs, shared, copies)
    wide = Heads(128, 256, rows, (qw_in, kvw_in), wide_refs, shared, copies)

    barrier = pltpu.get_barrier_semaphore()
    for t in (1, 2, 3):
        pl.semaphore_signal(barrier, inc=1, device_id={"z": (z + t) % 4}, device_id_type=pl.DeviceIdType.MESH)
        pl.semaphore_signal(barrier, inc=1, device_id={"x": (x + t) % 4}, device_id_type=pl.DeviceIdType.MESH)
    rank = narrow.rank
    for k in range(1, 8):
        r = (rank + k) % 8
        pl.semaphore_signal(barrier, inc=1, device_id={"y": r // 2, "c": r % 2}, device_id_type=pl.DeviceIdType.MESH)
    local = []
    for h in (narrow, wide):
        local.append(pltpu.make_async_copy(h.q_in, h.q_s.at[0], local_sems.at[len(local)]))
        local.append(pltpu.make_async_copy(h.kv_in.at[pl.ds(0, half)], h.kv_s.at[0, 0], local_sems.at[len(local)]))
    for c in local:
        c.start()
    pl.semaphore_wait(barrier, 13)

    narrow.send_swap()
    narrow.send_near()
    wide.send_swap()
    narrow.pass_swap()
    wide.send_near()

    pos, tab = narrow.pos, narrow.tab
    for i, t in enumerate(SHIFTS):
        pos[i] = (4 * ((z + 4 - t) % 4) + x) * rows
        n = (x + 4 - t) % 4
        pos[4 + i] = (4 * z + n) * rows
        pos[8 + i] = (4 * (3 - z) + n) * rows + half
    per = rows // TQ

    def list_q(qi, n):
        qp = pos[qi // per] + (qi % per) * TQ

        def list_k(kj, carry):
            n, first = carry
            p0, p1 = pos[4 + 2 * kj], pos[4 + 2 * kj + 1]
            hi, lo = jnp.maximum(p0, p1), jnp.minimum(p0, p1)
            full = hi + half - 1 <= qp
            some = lo <= qp + TQ - 1
            tab[0, n] = qi
            tab[1, n] = kj
            tab[2, n] = jnp.where(full, 0, 1)
            tab[3, n] = first
            return n + jnp.where(some, 1, 0), jnp.where(some, 0, first)
        m, _ = lax.fori_loop(0, 4, list_k, (n, 1))

        @pl.when(m == n)
        def _():
            tab[0, n] = qi
            tab[1, n] = 0
            tab[2, n] = 1
            tab[3, n] = 1
        return jnp.maximum(m, n + 1)
    steps = lax.fori_loop(0, 4 * per, list_q, 0)
    tab[3, steps] = 1

    narrow.relay_first()
    narrow.relay_second()
    wide.pass_swap()
    narrow.wait_all()
    for c in local:
        c.wait()
    narrow.prepare()
    narrow.run(steps, [wide.relay_first, wide.relay_second])
    narrow.send_stats()
    wide.wait_all()
    wide.prepare()
    narrow.mix_and_send(lam_ref[1, 0])
    narrow.mix(0, lam_ref[1, 0])
    wide.run(steps, [narrow.pass_parts, narrow.finish])
    wide.send_stats()
    wide.mix_and_send(lam_ref[0, 0])
    wide.pass_parts()
    wide.mix(0, lam_ref[0, 0])
    wide.finish()
    for h in (narrow, wide):
        for c in h.to_tokens:
            c.wait_recv()
    out_n[...] = narrow.out[...]
    out_w[...] = wide.out[...]
    for c in copies.all:
        c.wait_send()


def attention(qw, kw, vw, qn, kn, vn, lam):
    qw, kw, vw, qn, kn, vn = (a[:, 0] for a in (qw, kw, vw, qn, kn, vn))
    rows = qw.shape[0]
    half, mine = rows // 2, rows // 8

    def scratch(d, dv):
        return [
            pltpu.VMEM((4, rows, 2 * d), jnp.bfloat16),
            pltpu.VMEM((2, 4, half, 2 * d + dv), jnp.bfloat16),
            pltpu.VMEM((2 * d, 4 * rows), jnp.bfloat16),
            pltpu.VMEM((dv, 4 * rows), jnp.bfloat16),
            pltpu.VMEM((2, dv, 4 * rows), jnp.float32),
            pltpu.VMEM((4, 4 * rows), jnp.float32),
            pltpu.VMEM((3, 4, 4 * rows), jnp.float32),
            pltpu.VMEM((4, rows, dv), jnp.bfloat16),
            pltpu.VMEM((3, rows, dv), jnp.bfloat16),
            pltpu.VMEM((2, half, dv), jnp.bfloat16),
            pltpu.VMEM((rows, dv), jnp.bfloat16),
            pltpu.VMEM((mine, 8 * dv), jnp.bfloat16),
        ]
    any_ = pl.BlockSpec(memory_space=pl.ANY)
    vmem = pl.BlockSpec(memory_space=pltpu.VMEM)
    count = 2 * (2 + 2 + 1 + 8 + 3 + 6 + 7)
    return pl.pallas_call(
        functools.partial(attention_kernel, rows=rows),
        out_shape=(jax.ShapeDtypeStruct((mine, 8 * 256), jnp.bfloat16), jax.ShapeDtypeStruct((mine, 8 * 128), jnp.bfloat16)),
        in_specs=[pl.BlockSpec(memory_space=pltpu.SMEM)] + [any_] * 4,
        out_specs=(vmem, vmem),
        scratch_shapes=scratch(64, 128) + scratch(128, 256) + [
            pltpu.SMEM((4, 4 * (rows // TQ) * 4 + 1), jnp.int32),
            pltpu.SMEM((12,), jnp.int32),
            pltpu.VMEM((2, rows, TQ), jnp.float32),
            pltpu.VMEM((2, rows, TQ), jnp.float32),
            pltpu.VMEM((2, 8, TQ), jnp.float32),
            pltpu.VMEM((2, 8, TQ), jnp.float32),
            pltpu.VMEM((2, rows, TQ), jnp.bfloat16),
            pltpu.VMEM((2, TQ), jnp.float32),
            pltpu.VMEM((2, 8, TQ), jnp.float32),
            pltpu.SemaphoreType.DMA((count,)),
            pltpu.SemaphoreType.DMA((count,)),
            pltpu.SemaphoreType.DMA((4,)),
        ],
        name="attention",
        cost_estimate=pl.CostEstimate(flops=100 * 10**9, bytes_accessed=10**7, transcendentals=0),
        compiler_params=pltpu.CompilerParams(collective_id=0, has_side_effects=True, vmem_limit_bytes=60 * 2**20),
    )(lam, qn, jnp.concatenate([kn, vn], axis=1), qw, jnp.concatenate([kw, vw], axis=1))


def device_of(e):
    return {"z": e // 32, "x": (e // 8) % 4, "y": (e // 2) % 4, "c": e % 2}


def swapped(perm, rows):
    return jnp.dot(perm, rows, preferred_element_type=jnp.float32).astype(jnp.bfloat16)


def to_tiles(perm, block):
    width = block.shape[1] // 16
    stacked = jnp.concatenate([block[:, g * width:(g + 1) * width] for g in range(16)], axis=0)
    return swapped(perm, stacked).reshape(16, 16, width)


def experts_kernel(token_ref, slot_ref, weight_ref, normed_ref, stream_ref, gate_in, up_in, down_in, out_ref,
                   gate_s, up_s, down_s, perm_s, rows_s, stream_s, send_s, got_s, flat_s, hidden_s, back_s,
                   weight_sems, send_sems, recv_sems, send2_sems, recv2_sems):
    count = 128
    cap = send_s.shape[0] // count
    total = send_s.shape[0]
    tokens = normed_ref.shape[0]
    me = ((lax.axis_index("z") * 4 + lax.axis_index("x")) * 4 + lax.axis_index("y")) * 2 + lax.axis_index("c")
    loads = [
        pltpu.make_async_copy(src.at[0], dst, weight_sems.at[n])
        for n, (src, dst) in enumerate(((gate_in, gate_s), (up_in, up_s), (down_in, down_s)))
    ]
    for c in loads:
        c.start()
    barrier = pltpu.get_barrier_semaphore()

    def greet(k, _):
        pl.semaphore_signal(barrier, inc=1, device_id=device_of((me + k) % count), device_id_type=pl.DeviceIdType.MESH)
        return 0
    lax.fori_loop(1, count, greet, 0)

    r = lax.broadcasted_iota(jnp.int32, (256, 256), 0)
    c = lax.broadcasted_iota(jnp.int32, (256, 256), 1)
    perm_s[...] = jnp.where((r % 16) * 16 + r // 16 == c, 1.0, 0.0).astype(jnp.bfloat16)
    perm = perm_s[...]
    for b in range(tokens // 16):
        s = slice(b * 16, (b + 1) * 16)
        rows_s[s] = to_tiles(perm, normed_ref[s])

    def fill(n, _):
        for u in range(8):
            send_s[n * 8 + u] = rows_s[token_ref[n * 8 + u]]
        return 0
    lax.fori_loop(0, total // 8, fill, 0)
    pl.semaphore_wait(barrier, count - 1)

    def copy(src, dst, sends, recvs, k):
        e = (me + k) % count
        return pltpu.make_async_remote_copy(
            src_ref=src.at[pl.ds(e * cap, cap)],
            dst_ref=dst.at[pl.ds(me * cap, cap)],
            send_sem=sends.at[k],
            recv_sem=recvs.at[k],
            device_id=device_of(e),
            device_id_type=pl.DeviceIdType.MESH,
        )

    def exchange(src, dst, sends, recvs):
        def go(k, _):
            copy(src, dst, sends, recvs, k).start()
            return 0
        lax.fori_loop(1, count, go, 0)
        dst[pl.ds(me * cap, cap)] = src[pl.ds(me * cap, cap)]

    def arrive(src, dst, sends, recvs):
        def done(k, _):
            copy(src, dst, sends, recvs, k).wait_recv()
            return 0
        lax.fori_loop(1, count, done, 0)

    def leave(src, dst, sends, recvs):
        def done(k, _):
            copy(src, dst, sends, recvs, k).wait_send()
            return 0
        lax.fori_loop(1, count, done, 0)

    there = (send_s, got_s, send_sems, recv_sems)
    exchange(*there)
    for b in range(tokens // 16):
        s = slice(b * 16, (b + 1) * 16)
        stream_s[s] = to_tiles(perm, stream_ref[s])
    for c in loads:
        c.wait()
    arrive(*there)

    def flatten(n, _):
        for u in range(4):
            at = pl.multiple_of((n * 4 + u) * 16, 16)
            turned = swapped(perm, got_s[pl.ds(at, 16)].reshape(256, 128))
            for g in range(16):
                flat_s[pl.ds(at, 16), g * 128:(g + 1) * 128] = turned[g * 16:(g + 1) * 16]
        return 0
    lax.fori_loop(0, total // 64, flatten, 0)

    def first(n, _):
        at = pl.ds(pl.multiple_of(n * 256, 256), 256)
        gate = jnp.dot(flat_s[...], gate_s[:, at], preferred_element_type=jnp.float32)
        up = jnp.dot(flat_s[...], up_s[:, at], preferred_element_type=jnp.float32)
        hidden_s[:, at] = (gate * jax.nn.sigmoid(gate) * up).astype(jnp.bfloat16)
        return 0
    lax.fori_loop(0, hidden_s.shape[1] // 256, first, 0)

    def second(n, _):
        at = pl.ds(pl.multiple_of(n * 256, 256), 256)
        flat_s[:, at] = jnp.dot(hidden_s[...], down_s[:, at], preferred_element_type=jnp.float32).astype(jnp.bfloat16)
        return 0
    lax.fori_loop(0, flat_s.shape[1] // 256, second, 0)
    leave(*there)

    def unflatten(n, _):
        for u in range(4):
            at = pl.ds(pl.multiple_of((n * 4 + u) * 16, 16), 16)
            send_s[at] = to_tiles(perm, flat_s[at, :])
        return 0
    lax.fori_loop(0, total // 64, unflatten, 0)

    back = (send_s, back_s, send2_sems, recv2_sems)
    exchange(*back)
    arrive(*back)

    def combine(n, _):
        for u in range(4):
            t = n * 4 + u
            summed = weight_ref[2 * t] * back_s[slot_ref[2 * t]].astype(jnp.float32)
            summed = summed + weight_ref[2 * t + 1] * back_s[slot_ref[2 * t + 1]].astype(jnp.float32)
            rows_s[t] = (stream_s[t].astype(jnp.float32) + summed).astype(jnp.bfloat16)
        return 0
    lax.fori_loop(0, tokens // 4, combine, 0)
    for b in range(tokens // 16):
        s = slice(b * 16, (b + 1) * 16)
        turned = swapped(perm, rows_s[s].reshape(256, 128))
        for g in range(16):
            out_ref[s, g * 128:(g + 1) * 128] = turned[g * 16:(g + 1) * 16]
    leave(*back)


def experts(token_of_slot, slot_of_token, weight, normed, stream, gate, up, down):
    tokens, width = normed.shape
    slots = token_of_slot.shape[0]
    inner = gate.shape[2]
    smem = pl.BlockSpec(memory_space=pltpu.SMEM)
    vmem = pl.BlockSpec(memory_space=pltpu.VMEM)
    any_ = pl.BlockSpec(memory_space=pl.ANY)
    bf16 = jnp.bfloat16
    return pl.pallas_call(
        experts_kernel,
        out_shape=jax.ShapeDtypeStruct((tokens, width), bf16),
        in_specs=[smem] * 3 + [vmem] * 2 + [any_] * 3,
        out_specs=vmem,
        scratch_shapes=[
            pltpu.VMEM((width, inner), bf16),
            pltpu.VMEM((width, inner), bf16),
            pltpu.VMEM((inner, width), bf16),
            pltpu.VMEM((256, 256), bf16),
            pltpu.VMEM((tokens, 16, width // 16), bf16),
            pltpu.VMEM((tokens, 16, width // 16), bf16),
            pltpu.VMEM((slots, 16, width // 16), bf16),
            pltpu.VMEM((slots, 16, width // 16), bf16),
            pltpu.VMEM((slots, width), bf16),
            pltpu.VMEM((slots, inner), bf16),
            pltpu.VMEM((slots, 16, width // 16), bf16),
            pltpu.SemaphoreType.DMA((3,)),
            pltpu.SemaphoreType.DMA((128,)),
            pltpu.SemaphoreType.DMA((128,)),
            pltpu.SemaphoreType.DMA((128,)),
            pltpu.SemaphoreType.DMA((128,)),
        ],
        name="experts",
        cost_estimate=pl.CostEstimate(flops=50 * 10**9, bytes_accessed=2 * 10**7, transcendentals=0),
        compiler_params=pltpu.CompilerParams(collective_id=1, has_side_effects=True, vmem_limit_bytes=60 * 2**20),
    )(token_of_slot, slot_of_token, weight, normed, stream, gate, up, down)


def shards(
    query_wide,
    key_wide,
    value_wide,
    query_narrow,
    key_narrow,
    value_narrow,
    mix_lambda,
    residual_in,
    out_wide,
    out_narrow,
    ffn_gain,
    expert_ids,
    expert_weights,
    gate_weight,
    up_weight,
    down_weight,
):
    tok_count, local_heads, _ = query_wide.shape
    mine_wide, mine_narrow = attention(
        query_wide, key_wide, value_wide, query_narrow, key_narrow, value_narrow, mix_lambda
    )
    tp_size = lax.axis_size(TP)
    local_rows = tok_count // tp_size
    whole_wide, whole_narrow = (
        lax.all_gather(out_wide, TP, axis=0, tiled=True),
        lax.all_gather(out_narrow, TP, axis=0, tiled=True),
    )
    projected = jnp.dot(mine_wide, whole_wide, preferred_element_type=jnp.float32) + jnp.dot(
        mine_narrow, whole_narrow, preferred_element_type=jnp.float32
    )
    stream = (projected + residual_in.astype(jnp.float32)).astype(jnp.bfloat16)
    stream_f = stream.astype(jnp.float32)
    normed = (
        stream_f
        * lax.rsqrt(jnp.mean(stream_f * stream_f, axis=-1, keepdims=True) + 1e-06)
        * ffn_gain
    ).astype(jnp.bfloat16)
    experts_all = lax.axis_size(SP) * tp_size
    capacity = max(2, 4 * local_rows // experts_all)
    flat_expert = expert_ids.reshape(-1)
    expert_hot = (flat_expert[:, None] == jnp.arange(experts_all, dtype=jnp.int32)[None, :]).astype(
        jnp.int32
    )
    slot_rank = jnp.sum((jnp.cumsum(expert_hot, axis=0) - 1) * expert_hot, axis=1)
    flat_slot = flat_expert * capacity + slot_rank
    slot_ids = jnp.arange(experts_all * capacity, dtype=jnp.int32)
    placed = slot_ids[:, None] == flat_slot[None, :]
    token = jnp.arange(2 * local_rows, dtype=jnp.int32) // 2
    token_of_slot = jnp.max(jnp.where(placed, token[None, :], 0), axis=1)
    return experts(
        token_of_slot, flat_slot, expert_weights.reshape(-1), normed, stream, gate_weight, up_weight, down_weight
    )


def solution(mesh):
    finer = Mesh(mesh.devices.reshape(4, 4, 4, 2), ("z", "x", "y", "c"))
    placed = (
        P(SP, TP, None),
        P(SP, TP, None),
        P(SP, TP, None),
        P(SP, TP, None),
        P(SP, TP, None),
        P(SP, TP, None),
        P(None, TP),
        P(SP_TP, None),
        P(TP, None),
        P(TP, None),
        P(),
        P(SP_TP, None),
        P(SP_TP, None),
        P(SP_TP, None, None),
        P(SP_TP, None, None),
        P(SP_TP, None, None),
    )
    return jax.shard_map(
        shards, mesh=finer, in_specs=placed, out_specs=P(SP_TP, None), check_vma=False
    )
```

```python
import functools
import jax
import jax.numpy as jnp
from jax import lax
from jax.experimental import pallas as pl
from jax.experimental.pallas import tpu as pltpu
from jax.sharding import Mesh
from jax.sharding import PartitionSpec as P

TP = ("y", "c")
SP = ("z", "x")
SP_TP = ("z", "x", "y", "c")

NEG = -1e30
LOG2E = 1.4426950408889634
TQ = 256
CH = 256
SHIFTS = (0, 1, 3, 2)
SLOT = {t: i for i, t in enumerate(SHIFTS)}


class Copies:
    def __init__(self, send_sems, recv_sems):
        self.send_sems, self.recv_sems, self.count, self.all = send_sems, recv_sems, 0, []

    def one(self, src, dst, send, recv, device):
        return pltpu.make_async_remote_copy(
            src_ref=src,
            dst_ref=dst,
            send_sem=self.send_sems.at[send],
            recv_sem=self.recv_sems.at[recv],
            device_id=device,
            device_id_type=pl.DeviceIdType.MESH,
        )

    def make(self, src, dst, **device):
        copy = self.one(src, dst, self.count, self.count, device)
        self.count += 1
        self.all.append(copy)
        return copy


class Heads:
    def __init__(self, d, dv, rows, groups, ins, refs, kv_pair, shared, copies):
        self.d, self.dv, self.rows, self.half, self.groups = d, dv, rows, rows // 2, groups
        self.q_in, self.k_in, self.v_in = ins
        self.q_s, self.kv_s, self.qt_s, self.vt_s, self.acc, self.m_s, self.l_s, self.st, self.st_in, self.part, self.part_in, self.relay, self.heads, self.out = refs
        self.kv = kv_pair
        self.tab, self.pos, self.s_a, self.s_b, self.t_a, self.t_b, self.p_scr = shared
        self.scale = d ** (-0.5) * LOG2E
        self.copies = copies
        z, x = lax.axis_index("z"), lax.axis_index("x")
        up = {"z": (z + 1) % 4}, {"z": (z + 3) % 4}
        right = {"x": (x + 1) % 4}, {"x": (x + 3) % 4}
        half = self.half
        one, three, two = SLOT[1], SLOT[3], SLOT[2]
        h0, h1 = pl.ds(0, half), pl.ds(half, half)
        lanes = (self.k_in, pl.ds(0, 2 * d)), (self.v_in, pl.ds(2 * d, dv))
        self.q_near = [copies.make(self.q_in, self.q_s.at[one], **up[0]), copies.make(self.q_in, self.q_s.at[three], **up[1])]
        self.q_far = [
            copies.make(self.q_s.at[one, h0], self.q_s.at[two, h0], **up[0]),
            copies.make(self.q_s.at[three, h1], self.q_s.at[two, h1], **up[1]),
        ]
        self.swap = [copies.make(src.at[h1], self.kv_at(1, 0, slice(None), at), z=3 - z) for src, at in lanes]
        self.own = [(src.at[h0], self.kv_at(0, 0, slice(None), at)) for src, at in lanes] + [(self.q_in, self.q_s.at[0])]
        quarter = half // 2
        g0, g1 = pl.ds(0, quarter), pl.ds(quarter, quarter)
        self.kv_near = [
            [[copies.make(src.at[h0], self.kv_at(0, slot, slice(None), at), **to) for src, at in lanes] for slot, to in ((one, right[0]), (three, right[1]))],
            [[copies.make(self.kv_at(1, 0), self.kv_at(1, slot), **to)] for slot, to in ((one, right[0]), (three, right[1]))],
        ]
        self.kv_far = [[
            copies.make(self.kv_at(b, one, g0), self.kv_at(b, two, g0), **right[0]),
            copies.make(self.kv_at(b, three, g1), self.kv_at(b, two, g1), **right[1]),
        ] for b in range(2)]
        self.st_out, self.part_near, self.part_first, self.part_far = [], [], [], []
        for p0, p1 in groups:
            cols = pl.ds(p0 * 4 * TQ, (p1 - p0) * 4 * TQ)
            self.st_out.append([copies.make(self.st.at[:, cols], self.st_in.at[t - 1, :, cols], z=(z + t) % 4) for t in (1, 2, 3)])
            size = (p1 - p0) * TQ
            all_, f0, f1 = pl.ds(p0 * TQ, size), pl.ds(p0 * TQ, size // 2), pl.ds(p0 * TQ + size // 2, size // 2)
            held = pl.ds(p0 * TQ // 2, size // 2)
            self.part_near.append([
                copies.make(self.part.at[one, all_], self.part_in.at[0, all_], **up[1]),
                copies.make(self.part.at[three, all_], self.part_in.at[1, all_], **up[0]),
            ])
            self.part_first.append([
                copies.make(self.part.at[two, f0], self.relay.at[0, held], **up[0]),
                copies.make(self.part.at[two, f1], self.relay.at[1, held], **up[1]),
            ])
            self.part_far.append([
                copies.make(self.relay.at[0, held], self.part_in.at[2, f0], **up[0]),
                copies.make(self.relay.at[1, held], self.part_in.at[2, f1], **up[1]),
            ])
        self.rank = lax.axis_index("y") * 2 + lax.axis_index("c")
        self.base = copies.count
        copies.count += 8

    def kv_at(self, b, *index):
        ref = self.kv[b] if self.kv else self.kv_s
        index = index if self.kv else (b,) + index
        return ref.at[index] if index else ref

    def to_token(self, r):
        mine = self.rows // 8
        at = pl.multiple_of(self.rank * self.dv, self.dv)
        return self.copies.one(
            self.heads.at[pl.ds(r * mine, mine)], self.out.at[:, pl.ds(at, self.dv)],
            self.base + r, self.base + self.rank, {"y": r // 2, "c": r % 2},
        )

    def from_rank(self, r):
        mine = self.rows // 8
        return self.copies.one(
            self.heads.at[pl.ds(r * mine, mine)], self.out.at[:, r * self.dv:(r + 1) * self.dv],
            self.base + r, self.base + r, {"y": r // 2, "c": r % 2},
        )

    def send_swap(self):
        for c in self.swap:
            c.start()

    def send_near(self):
        for c in self.kv_near[0][0] + self.kv_near[0][1] + self.q_near:
            c.start()

    def pass_swap(self):
        for c in self.swap:
            c.wait_recv()
        for near in self.kv_near[1]:
            near[0].start()

    def relay_queries(self):
        for near, far in zip(self.q_near, self.q_far):
            near.wait_recv()
            far.start()

    def relay_keys(self, b):
        for near, far in zip(self.kv_near[b], self.kv_far[b]):
            for c in near:
                c.wait_recv()
            far.start()

    def clear(self):
        self.m_s[...] = jnp.full_like(self.m_s, NEG)
        self.l_s[...] = jnp.zeros_like(self.l_s)

        def tile(n, _):
            self.acc[:, :, pl.ds(pl.multiple_of(n * TQ, TQ), TQ)] = jnp.zeros((2, self.dv, TQ), jnp.float32)
            return 0
        lax.fori_loop(0, 4 * self.rows // TQ, tile, 0)

    def turn_queries(self):
        for c in self.q_far:
            c.wait_recv()

        def turn(i, _):
            for p in range(self.rows // TQ):
                at = pl.multiple_of((p * 4 + i) * TQ, TQ)
                self.qt_s[:, pl.ds(at, TQ)] = self.q_s[i, p * TQ:(p + 1) * TQ].T
            return 0
        lax.fori_loop(0, 4, turn, 0)

    def wait_values(self, b):
        for c in self.kv_far[b]:
            c.wait_recv()

    def turn_values(self, b):
        d, dv, half = self.d, self.dv, self.half

        def turn(i, _):
            at = pl.multiple_of((b * 4 + i) * half, half)
            self.vt_s[:, pl.ds(at, half)] = self.kv_at(b)[i, :, 2 * d:2 * d + dv].T
            return 0
        lax.fori_loop(0, 4, turn, 0)

    def read(self, i, s_buf, t_buf, b=None):
        d, half = self.d, self.half
        q0 = pl.multiple_of(self.tab[0, i] * TQ, TQ)
        kj = self.tab[1, i]
        part, first = kj // 2, (kj % 2) * 2
        for w in range(2):
            qt = self.qt_s[w * d:(w + 1) * d, pl.ds(q0, TQ)]
            top = None
            for c in range(2):
                lanes = slice(w * d, (w + 1) * d)
                k = self.kv_s[part, first + c, :, lanes] if b is None else self.kv[b][first + c, :, lanes]
                s = jnp.dot(k, qt, preferred_element_type=jnp.float32)
                s_buf[w, c * half:(c + 1) * half] = s
                m8 = jnp.max(s.reshape(half // 8, 8, TQ), axis=0)
                top = m8 if top is None else jnp.maximum(top, m8)
            t_buf[w] = top

    def mask(self, i, s_buf, t_buf):
        rows, half = self.rows, self.half
        qi, kj = self.tab[0, i], self.tab[1, i]
        qp = self.pos[qi % 4] + (qi // 4) * TQ
        CM = 128
        t_buf[...] = jnp.full_like(t_buf, NEG)

        def chunk(c, _):
            r = pl.multiple_of(c * CM, CM)
            late = c // (half // CM)
            k0 = self.pos[4 + 2 * kj + late] + (c - late * (half // CM)) * CM
            keep = lax.broadcasted_iota(jnp.int32, (CM, TQ), 0) - lax.broadcasted_iota(jnp.int32, (CM, TQ), 1) <= qp - k0
            for w in range(2):
                s = jnp.where(keep, s_buf[w, pl.ds(r, CM)], NEG)
                s_buf[w, pl.ds(r, CM)] = s
                t_buf[w] = jnp.maximum(t_buf[w], jnp.max(s.reshape(CM // 8, 8, TQ), axis=0))
            return 0
        lax.fori_loop(0, rows // CM, chunk, 0)

    def weigh(self, i, s_buf, t_buf):
        rows = self.rows
        cols = pl.ds(pl.multiple_of(self.tab[0, i] * TQ, TQ), TQ)
        k0 = pl.multiple_of(self.tab[1, i] * rows, rows)
        for w in range(2):
            old = self.m_s[w:w + 1, cols]
            new = jnp.maximum(old, jnp.max(t_buf[w], axis=0, keepdims=True) * self.scale)
            f = jnp.exp2(old - new)
            self.m_s[w:w + 1, cols] = new
            tot = None
            for c in range(rows // CH):
                p = jnp.exp2(s_buf[w, c * CH:(c + 1) * CH] * self.scale - new)
                t8 = jnp.sum(p.reshape(CH // 8, 8, TQ), axis=0)
                tot = t8 if tot is None else tot + t8
                self.p_scr[w, c * CH:(c + 1) * CH] = p.astype(jnp.bfloat16)
            o = jnp.dot(self.vt_s[:, pl.ds(k0, rows)], self.p_scr[w], preferred_element_type=jnp.float32)
            self.l_s[w, :, cols] = self.l_s[w, :, cols] * f + tot
            self.acc[w, :, cols] = self.acc[w, :, cols] * f + o

    def run(self, low, high, hooks, b=None):
        def advance(i, cur, nxt):
            @pl.when(self.tab[2, i] == 1)
            def _():
                self.mask(i, *cur)
            self.read(jnp.minimum(i + 1, high - 1), *nxt, b)
            self.weigh(i, *cur)

        one, two = (self.s_a, self.t_a), (self.s_b, self.t_b)
        self.read(low, *one, b)
        turns = jnp.maximum((high - low + 1) // 2, len(hooks) + 1)

        def pair(n, _):
            for k, hook in enumerate(hooks):
                pl.when(n == turns * (k + 1) // (len(hooks) + 1))(hook)
            i = low + 2 * n

            @pl.when(i < high)
            def _():
                advance(i, one, two)

            @pl.when(i + 1 < high)
            def _():
                advance(i + 1, two, one)
            return 0
        lax.fori_loop(0, turns, pair, 0)

    def mix(self, g, slot, lam):
        dv = self.dv
        for p in range(*self.groups[g]):
            c0 = (p * 4 + slot) * TQ
            stats = [self.st[:, c0:c0 + TQ]]
            for t in (1, 2, 3):
                at = (p * 4 + SLOT[(SHIFTS[slot] - t) % 4]) * TQ
                stats.append(self.st_in[t - 1, :, at:at + TQ])
            weights = []
            for w in range(2):
                peaks = [s[w:w + 1] for s in stats]
                top = functools.reduce(jnp.maximum, peaks)
                total = sum(s[2 + w:3 + w] * jnp.exp2(m - top) for m, s in zip(peaks, stats))
                weights.append(jnp.exp2(peaks[0] - top) / total)
            mixed = self.acc[0, :, c0:c0 + TQ] * weights[0] - self.acc[1, :, c0:c0 + TQ] * (weights[1] * lam)
            self.part[slot, p * TQ:(p + 1) * TQ] = mixed.T.astype(jnp.bfloat16)

    def send_stats(self, g):
        p0, p1 = self.groups[g]
        cols = slice(p0 * 4 * TQ, p1 * 4 * TQ)
        self.st[0:2, cols] = self.m_s[:, cols]
        for w in range(2):
            self.st[2 + w:3 + w, cols] = jnp.sum(self.l_s[w, :, cols], axis=0, keepdims=True)
        for c in self.st_out[g]:
            c.start()

    def mix_and_send(self, g, lam):
        for c in self.st_out[g]:
            c.wait_recv()
        self.mix(g, SLOT[2], lam)
        for c in self.part_first[g]:
            c.start()
        self.mix(g, SLOT[1], lam)
        self.part_near[g][0].start()
        self.mix(g, SLOT[3], lam)
        self.part_near[g][1].start()

    def pass_parts(self, g):
        for first, far in zip(self.part_first[g], self.part_far[g]):
            first.wait_recv()
            far.start()

    def finish(self, g, lam):
        self.mix(g, 0, lam)
        for c in self.part_near[g] + self.part_far[g]:
            c.wait_recv()
        B = 128
        p0, p1 = self.groups[g]
        for at in range(p0 * TQ, p1 * TQ, B):
            r = slice(at, at + B)
            total = self.part[0, r].astype(jnp.float32)
            for n in range(3):
                total = total + self.part_in[n, r].astype(jnp.float32)
            total = total * lax.rsqrt(jnp.mean(total * total, axis=-1, keepdims=True) + 1e-06)
            self.heads[r] = total.astype(jnp.bfloat16)
        mine = self.rows // 8
        for r in range(8):
            if p0 * TQ < (r + 1) * mine <= p1 * TQ:
                pl.when(r != self.rank)(self.to_token(r).start)


class Weights:
    def __init__(self, ins, sizes, held, copies):
        self.held = held
        y, c = lax.axis_index("y"), lax.axis_index("c")
        up, down, pair = {"y": (y + 1) % 4}, {"y": (y + 3) % 4}, {"c": 1 - c}
        self.own, self.first, self.near, self.far, self.pass_near, self.pass_far = [], [], [], [], [], []
        base = 0
        for src, size in zip(ins, sizes):
            half = size // 2

            def rows(t, at=0, n=size, base=base, size=size):
                return held.at[pl.ds(pl.multiple_of(base + (((y + t) % 4) * 2 + c) * size + at, half), n)]
            self.own.append((src, rows(0)))
            self.first.append(copies.make(src, rows(0), **pair))
            self.near.append([copies.make(src, rows(0), **up), copies.make(src, rows(0), **down)])
            self.far.append([
                copies.make(rows(3, 0, half), rows(3, 0, half), **up),
                copies.make(rows(1, half, half), rows(1, half, half), **down),
            ])
            self.pass_near.append([copies.make(rows(3), rows(3), **pair), copies.make(rows(1), rows(1), **pair)])
            self.pass_far.append([copies.make(rows(2, 0, half), rows(2, 0, half), **pair), copies.make(rows(2, half, half), rows(2, half, half), **pair)])
            base += 8 * size

    def send(self):
        for near, first in zip(self.near, self.first):
            for c in near:
                c.start()
            first.start()

    def relay(self):
        for near, far, onward in zip(self.near, self.far, self.pass_near):
            for n, f, o in zip(near, far, onward):
                n.wait_recv()
                f.start()
                o.start()

    def last(self):
        for far, onward in zip(self.far, self.pass_far):
            for f, o in zip(far, onward):
                f.wait_recv()
                o.start()

    def wait(self):
        for c in self.first:
            c.wait_recv()
        for group in self.pass_near + self.pass_far:
            for c in group:
                c.wait_recv()


def attention_kernel(lam_ref, residual_ref, gain_ref, ow_in, on_in, qn_in, kn_in, vn_in, qw_in, kw_in, vw_in, stream_ref, normed_ref, *scratch, rows):
    narrow_refs, wide_refs = scratch[:14], scratch[14:28]
    shared, (send_sems, recv_sems, local_sems, weights_s, sum_s) = scratch[28:35], scratch[35:40]
    z, x = lax.axis_index("z"), lax.axis_index("x")
    half = rows // 2
    per = rows // TQ
    copies = Copies(send_sems, recv_sems)
    narrow = Heads(64, 128, rows, ((0, per - 1), (per - 1, per)), (qn_in, kn_in, vn_in), narrow_refs, None, shared, copies)
    wide = Heads(128, 256, rows, ((0, per),), (qw_in, kw_in, vw_in), wide_refs, scratch[40:42], shared, copies)
    weights = Weights((ow_in, on_in), (256, 128), weights_s, copies)
    lam_w, lam_n = lam_ref[0], lam_ref[1]

    barrier = pltpu.get_barrier_semaphore()
    for t in (1, 2, 3):
        pl.semaphore_signal(barrier, inc=1, device_id={"z": (z + t) % 4}, device_id_type=pl.DeviceIdType.MESH)
        pl.semaphore_signal(barrier, inc=1, device_id={"x": (x + t) % 4}, device_id_type=pl.DeviceIdType.MESH)
    rank = narrow.rank
    for k in range(1, 8):
        r = (rank + k) % 8
        pl.semaphore_signal(barrier, inc=1, device_id={"y": r // 2, "c": r % 2}, device_id_type=pl.DeviceIdType.MESH)
    local = []
    for h in (narrow, wide):
        for src, dst in h.own:
            local.append(pltpu.make_async_copy(src, dst, local_sems.at[len(local)]))
    for src, dst in weights.own:
        local.append(pltpu.make_async_copy(src, dst, local_sems.at[len(local)]))
    for c in local:
        c.start()
    pl.semaphore_wait(barrier, 13)

    wide.send_swap()
    wide.send_near()
    narrow.send_swap()
    weights.send()
    wide.clear()

    pos, tab = narrow.pos, narrow.tab
    for i, t in enumerate(SHIFTS):
        pos[i] = (4 * ((z + 4 - t) % 4) + x) * rows
        n = (x + 4 - t) % 4
        pos[4 + i] = (4 * z + n) * rows
        pos[8 + i] = (4 * (3 - z) + n) * rows + half

    def list_steps(p0, p1, k0, k1, n):
        def list_q(j, n):
            qi = 4 * p0 + j
            qp = pos[qi % 4] + (qi // 4) * TQ

            def list_k(kj, n):
                first, second = pos[4 + 2 * kj], pos[5 + 2 * kj]
                hi, lo = jnp.maximum(first, second), jnp.minimum(first, second)
                tab[0, n] = qi
                tab[1, n] = kj
                tab[2, n] = jnp.where(hi + half - 1 <= qp, 0, 1)
                return n + jnp.where(lo <= qp + TQ - 1, 1, 0)
            return lax.fori_loop(k0, k1, list_k, n)
        return lax.fori_loop(0, 4 * (p1 - p0), list_q, n)
    wide_a = list_steps(0, per, 0, 2, 0)
    wide_b = list_steps(0, per, 2, 4, wide_a)
    narrow_a = list_steps(0, per - 1, 0, 4, wide_b)
    narrow_b = list_steps(per - 1, per, 0, 4, narrow_a)
    for n in range(3):
        tab[n, narrow_b] = 0

    for c in local:
        c.wait()
    wide.relay_keys(0)
    wide.relay_queries()
    wide.pass_swap()
    narrow.send_near()
    narrow.clear()
    wide.turn_queries()
    wide.wait_values(0)
    wide.turn_values(0)

    def narrow_relays():
        narrow.relay_queries()
        narrow.relay_keys(0)
    wide.run(0, wide_a, [narrow.pass_swap, lambda: wide.relay_keys(1)], 0)
    wide.wait_values(1)
    wide.turn_values(1)
    wide.run(wide_a, wide_b, [narrow_relays, lambda: narrow.relay_keys(1)], 1)
    wide.send_stats(0)
    for b in range(2):
        narrow.wait_values(b)
    narrow.turn_queries()
    narrow.turn_values(0)
    narrow.turn_values(1)
    narrow.run(wide_b, narrow_a, [lambda: wide.mix_and_send(0, lam_w), weights.relay, lambda: wide.pass_parts(0)])
    narrow.send_stats(0)
    narrow.run(narrow_a, narrow_b, [lambda: narrow.mix_and_send(0, lam_n)])
    narrow.send_stats(1)
    wide.finish(0, lam_w)
    narrow.pass_parts(0)
    narrow.mix_and_send(1, lam_n)
    weights.last()
    narrow.finish(0, lam_n)
    narrow.pass_parts(1)
    mine = rows // 8
    width = weights_s.shape[1]

    def collect(h):
        for r in range(8):
            pl.when(r != rank)(h.from_rank(r).wait_recv)
        at = pl.multiple_of(rank * mine, mine)
        h.out[:, pl.ds(pl.multiple_of(rank * h.dv, h.dv), h.dv)] = h.heads[pl.ds(at, mine)]
    narrow.finish(1, lam_n)
    weights.wait()
    collect(wide)
    edge = 8 * wide.dv

    def project_wide(n, _):
        at = pl.ds(pl.multiple_of(n * 512, 512), 512)
        sum_s[:, at] = jnp.dot(wide.out[...], weights_s[0:edge, at], preferred_element_type=jnp.float32)
        return 0
    lax.fori_loop(0, width // 512, project_wide, 0)
    collect(narrow)

    def project(n, square):
        at = pl.ds(pl.multiple_of(n * 512, 512), 512)
        total = sum_s[:, at] + jnp.dot(narrow.out[...], weights_s[edge:, at], preferred_element_type=jnp.float32)
        stream = (total + residual_ref[:, at].astype(jnp.float32)).astype(jnp.bfloat16)
        stream_ref[:, at] = stream
        stream = stream.astype(jnp.float32)
        return square + jnp.sum(stream * stream, axis=-1, keepdims=True)
    square = lax.fori_loop(0, width // 512, project, jnp.zeros((mine, 1), jnp.float32))
    factor = lax.rsqrt(square / width + 1e-06)

    def norm(n, _):
        at = pl.ds(pl.multiple_of(n * 512, 512), 512)
        normed_ref[:, at] = (stream_ref[:, at].astype(jnp.float32) * factor * gain_ref[:, at]).astype(jnp.bfloat16)
        return 0
    lax.fori_loop(0, width // 512, norm, 0)
    for h in (narrow, wide):
        for r in range(8):
            pl.when(r != rank)(h.to_token(r).wait_send)
    for c in copies.all:
        c.wait_send()


def attention(qw, kw, vw, qn, kn, vn, lam, residual, out_w, out_n, gain):
    qw, kw, vw, qn, kn, vn = (a[:, 0] for a in (qw, kw, vw, qn, kn, vn))
    rows = qw.shape[0]
    half, mine = rows // 2, rows // 8
    total = 4 * rows
    bf16, f32 = jnp.bfloat16, jnp.float32

    def scratch(d, dv, both):
        return [
            pltpu.VMEM((4, rows, 2 * d), bf16),
            pltpu.VMEM((2, 4, half, 2 * d + dv) if both else (16, 128), bf16),
            pltpu.VMEM((2 * d, total), bf16),
            pltpu.VMEM((dv, total), bf16),
            pltpu.VMEM((2, dv, total), f32),
            pltpu.VMEM((2, total), f32),
            pltpu.VMEM((2, 8, total), f32),
            pltpu.VMEM((4, total), f32),
            pltpu.VMEM((3, 4, total), f32),
            pltpu.VMEM((4, rows, dv), bf16),
            pltpu.VMEM((3, rows, dv), bf16),
            pltpu.VMEM((2, half, dv), bf16),
            pltpu.VMEM((rows, dv), bf16),
            pltpu.VMEM((mine, 8 * dv), bf16),
        ]
    any_ = pl.BlockSpec(memory_space=pl.ANY)
    vmem = pl.BlockSpec(memory_space=pltpu.VMEM)
    count = 2 * (4 + 2 + 4 + 2 + 4 + 8) + 3 * 9 + 2 * 9
    width = residual.shape[1]
    return pl.pallas_call(
        functools.partial(attention_kernel, rows=rows),
        out_shape=(jax.ShapeDtypeStruct((mine, width), bf16),) * 2,
        in_specs=[pl.BlockSpec(memory_space=pltpu.SMEM), vmem, vmem] + [any_] * 8,
        out_specs=(vmem, vmem),
        scratch_shapes=scratch(64, 128, True) + scratch(128, 256, False) + [
            pltpu.SMEM((3, 2 * 4 * (rows // TQ) * 4 + 1), jnp.int32),
            pltpu.SMEM((12,), jnp.int32),
            pltpu.VMEM((2, rows, TQ), f32),
            pltpu.VMEM((2, rows, TQ), f32),
            pltpu.VMEM((2, 8, TQ), f32),
            pltpu.VMEM((2, 8, TQ), f32),
            pltpu.VMEM((2, rows, TQ), bf16),
            pltpu.SemaphoreType.DMA((count,)),
            pltpu.SemaphoreType.DMA((count,)),
            pltpu.SemaphoreType.DMA((8,)),
            pltpu.VMEM((8 * 384, width), bf16),
            pltpu.VMEM((mine, width), f32),
            pltpu.VMEM((4, half, 512), bf16),
            pltpu.VMEM((4, half, 512), bf16),
        ],
        name="attention",
        cost_estimate=pl.CostEstimate(flops=100 * 10**9, bytes_accessed=10**7, transcendentals=0),
        compiler_params=pltpu.CompilerParams(collective_id=0, has_side_effects=True, vmem_limit_bytes=60 * 2**20),
    )(lam.reshape(-1), residual, gain.reshape(1, -1), out_w, out_n, qn, kn, vn, qw, kw, vw)


def device_of(e):
    return {"z": e // 32, "x": (e // 8) % 4, "y": (e // 2) % 4, "c": e % 2}


def swapped(perm, rows):
    return jnp.dot(perm, rows, preferred_element_type=jnp.float32).astype(jnp.bfloat16)


def to_tiles(perm, block):
    width = block.shape[1] // 16
    stacked = jnp.concatenate([block[:, g * width:(g + 1) * width] for g in range(16)], axis=0)
    return swapped(perm, stacked).reshape(16, 16, width)


def experts_kernel(token_ref, slot_ref, weight_ref, normed_ref, stream_ref, gate_in, up_in, down_in, out_ref,
                   gate_s, up_s, down_s, perm_s, rows_s, stream_s, send_s, got_s, flat_s, hidden_s, back_s,
                   weight_sems, send_sems, recv_sems, send2_sems, recv2_sems):
    count = 128
    cap = send_s.shape[0] // count
    total = send_s.shape[0]
    tokens = normed_ref.shape[0]
    me = ((lax.axis_index("z") * 4 + lax.axis_index("x")) * 4 + lax.axis_index("y")) * 2 + lax.axis_index("c")
    loads = [
        pltpu.make_async_copy(src.at[0], dst, weight_sems.at[n])
        for n, (src, dst) in enumerate(((gate_in, gate_s), (up_in, up_s), (down_in, down_s)))
    ]
    for c in loads:
        c.start()
    barrier = pltpu.get_barrier_semaphore()

    def greet(k, _):
        pl.semaphore_signal(barrier, inc=1, device_id=device_of((me + k) % count), device_id_type=pl.DeviceIdType.MESH)
        return 0
    lax.fori_loop(1, count, greet, 0)

    r = lax.broadcasted_iota(jnp.int32, (256, 256), 0)
    c = lax.broadcasted_iota(jnp.int32, (256, 256), 1)
    perm_s[...] = jnp.where((r % 16) * 16 + r // 16 == c, 1.0, 0.0).astype(jnp.bfloat16)
    perm = perm_s[...]
    for b in range(tokens // 16):
        s = slice(b * 16, (b + 1) * 16)
        rows_s[s] = to_tiles(perm, normed_ref[s])

    def fill(n, _):
        for u in range(8):
            send_s[n * 8 + u] = rows_s[token_ref[n * 8 + u]]
        return 0
    lax.fori_loop(0, total // 8, fill, 0)
    pl.semaphore_wait(barrier, count - 1)

    def copy(src, dst, sends, recvs, k):
        e = (me + k) % count
        return pltpu.make_async_remote_copy(
            src_ref=src.at[pl.ds(e * cap, cap)],
            dst_ref=dst.at[pl.ds(me * cap, cap)],
            send_sem=sends.at[k],
            recv_sem=recvs.at[k],
            device_id=device_of(e),
            device_id_type=pl.DeviceIdType.MESH,
        )

    def exchange(src, dst, sends, recvs):
        def go(k, _):
            copy(src, dst, sends, recvs, (k * 53) % 128).start()
            return 0
        lax.fori_loop(1, count, go, 0)
        dst[pl.ds(me * cap, cap)] = src[pl.ds(me * cap, cap)]

    def arrive(src, dst, sends, recvs):
        def done(k, _):
            copy(src, dst, sends, recvs, k).wait_recv()
            return 0
        lax.fori_loop(1, count, done, 0)

    def leave(src, dst, sends, recvs):
        def done(k, _):
            copy(src, dst, sends, recvs, k).wait_send()
            return 0
        lax.fori_loop(1, count, done, 0)

    there = (send_s, got_s, send_sems, recv_sems)
    exchange(*there)
    for b in range(tokens // 16):
        s = slice(b * 16, (b + 1) * 16)
        stream_s[s] = to_tiles(perm, stream_ref[s])
    for c in loads:
        c.wait()
    arrive(*there)

    def flatten(n, _):
        for u in range(4):
            at = pl.multiple_of((n * 4 + u) * 16, 16)
            turned = swapped(perm, got_s[pl.ds(at, 16)].reshape(256, 128))
            for g in range(16):
                flat_s[pl.ds(at, 16), g * 128:(g + 1) * 128] = turned[g * 16:(g + 1) * 16]
        return 0
    lax.fori_loop(0, total // 64, flatten, 0)

    def first(n, _):
        at = pl.ds(pl.multiple_of(n * 256, 256), 256)
        gate = jnp.dot(flat_s[...], gate_s[:, at], preferred_element_type=jnp.float32)
        up = jnp.dot(flat_s[...], up_s[:, at], preferred_element_type=jnp.float32)
        hidden_s[:, at] = (gate * jax.nn.sigmoid(gate) * up).astype(jnp.bfloat16)
        return 0
    lax.fori_loop(0, hidden_s.shape[1] // 256, first, 0)

    def second(n, _):
        at = pl.ds(pl.multiple_of(n * 256, 256), 256)
        flat_s[:, at] = jnp.dot(hidden_s[...], down_s[:, at], preferred_element_type=jnp.float32).astype(jnp.bfloat16)
        return 0
    lax.fori_loop(0, flat_s.shape[1] // 256, second, 0)
    leave(*there)

    def unflatten(n, _):
        for u in range(4):
            at = pl.ds(pl.multiple_of((n * 4 + u) * 16, 16), 16)
            send_s[at] = to_tiles(perm, flat_s[at, :])
        return 0
    lax.fori_loop(0, total // 64, unflatten, 0)

    back = (send_s, back_s, send2_sems, recv2_sems)
    exchange(*back)
    arrive(*back)

    def combine(n, _):
        for u in range(4):
            t = n * 4 + u
            summed = weight_ref[2 * t] * back_s[slot_ref[2 * t]].astype(jnp.float32)
            summed = summed + weight_ref[2 * t + 1] * back_s[slot_ref[2 * t + 1]].astype(jnp.float32)
            rows_s[t] = (stream_s[t].astype(jnp.float32) + summed).astype(jnp.bfloat16)
        return 0
    lax.fori_loop(0, tokens // 4, combine, 0)
    for b in range(tokens // 16):
        s = slice(b * 16, (b + 1) * 16)
        turned = swapped(perm, rows_s[s].reshape(256, 128))
        for g in range(16):
            out_ref[s, g * 128:(g + 1) * 128] = turned[g * 16:(g + 1) * 16]
    leave(*back)


def experts(token_of_slot, slot_of_token, weight, normed, stream, gate, up, down):
    tokens, width = normed.shape
    slots = token_of_slot.shape[0]
    inner = gate.shape[2]
    smem = pl.BlockSpec(memory_space=pltpu.SMEM)
    vmem = pl.BlockSpec(memory_space=pltpu.VMEM)
    any_ = pl.BlockSpec(memory_space=pl.ANY)
    bf16 = jnp.bfloat16
    return pl.pallas_call(
        experts_kernel,
        out_shape=jax.ShapeDtypeStruct((tokens, width), bf16),
        in_specs=[smem] * 3 + [vmem] * 2 + [any_] * 3,
        out_specs=vmem,
        scratch_shapes=[
            pltpu.VMEM((width, inner), bf16),
            pltpu.VMEM((width, inner), bf16),
            pltpu.VMEM((inner, width), bf16),
            pltpu.VMEM((256, 256), bf16),
            pltpu.VMEM((tokens, 16, width // 16), bf16),
            pltpu.VMEM((tokens, 16, width // 16), bf16),
            pltpu.VMEM((slots, 16, width // 16), bf16),
            pltpu.VMEM((slots, 16, width // 16), bf16),
            pltpu.VMEM((slots, width), bf16),
            pltpu.VMEM((slots, inner), bf16),
            pltpu.VMEM((slots, 16, width // 16), bf16),
            pltpu.SemaphoreType.DMA((3,)),
            pltpu.SemaphoreType.DMA((128,)),
            pltpu.SemaphoreType.DMA((128,)),
            pltpu.SemaphoreType.DMA((128,)),
            pltpu.SemaphoreType.DMA((128,)),
        ],
        name="experts",
        cost_estimate=pl.CostEstimate(flops=50 * 10**9, bytes_accessed=2 * 10**7, transcendentals=0),
        compiler_params=pltpu.CompilerParams(collective_id=1, has_side_effects=True, vmem_limit_bytes=60 * 2**20),
    )(token_of_slot, slot_of_token, weight, normed, stream, gate, up, down)


def shards(
    query_wide,
    key_wide,
    value_wide,
    query_narrow,
    key_narrow,
    value_narrow,
    mix_lambda,
    residual_in,
    out_wide,
    out_narrow,
    ffn_gain,
    expert_ids,
    expert_weights,
    gate_weight,
    up_weight,
    down_weight,
):
    tok_count, local_heads, _ = query_wide.shape
    stream, normed = attention(
        query_wide, key_wide, value_wide, query_narrow, key_narrow, value_narrow, mix_lambda,
        residual_in, out_wide, out_narrow, ffn_gain,
    )
    tp_size = lax.axis_size(TP)
    local_rows = tok_count // tp_size
    experts_all = lax.axis_size(SP) * tp_size
    capacity = max(2, 4 * local_rows // experts_all)
    flat_expert = expert_ids.reshape(-1)
    expert_hot = (flat_expert[:, None] == jnp.arange(experts_all, dtype=jnp.int32)[None, :]).astype(
        jnp.int32
    )
    slot_rank = jnp.sum((jnp.cumsum(expert_hot, axis=0) - 1) * expert_hot, axis=1)
    flat_slot = flat_expert * capacity + slot_rank
    slot_ids = jnp.arange(experts_all * capacity, dtype=jnp.int32)
    placed = slot_ids[:, None] == flat_slot[None, :]
    token = jnp.arange(2 * local_rows, dtype=jnp.int32) // 2
    token_of_slot = jnp.max(jnp.where(placed, token[None, :], 0), axis=1)
    return experts(
        token_of_slot, flat_slot, expert_weights.reshape(-1), normed, stream, gate_weight, up_weight, down_weight
    )


def solution(mesh):
    finer = Mesh(mesh.devices.reshape(4, 4, 4, 2), ("z", "x", "y", "c"))
    placed = (
        P(SP, TP, None),
        P(SP, TP, None),
        P(SP, TP, None),
        P(SP, TP, None),
        P(SP, TP, None),
        P(SP, TP, None),
        P(None, TP),
        P(SP_TP, None),
        P(TP, None),
        P(TP, None),
        P(),
        P(SP_TP, None),
        P(SP_TP, None),
        P(SP_TP, None, None),
        P(SP_TP, None, None),
        P(SP_TP, None, None),
    )
    return jax.shard_map(
        shards, mesh=finer, in_specs=placed, out_specs=P(SP_TP, None), check_vma=False
    )
```

```python
import functools
import jax
import jax.numpy as jnp
from jax import lax
from jax.experimental import pallas as pl
from jax.experimental.pallas import tpu as pltpu
from jax.sharding import Mesh
from jax.sharding import PartitionSpec as P

TP = ("y", "c")
SP = ("z", "x")
SP_TP = ("z", "x", "y", "c")

NEG = -1e30
LOG2E = 1.4426950408889634
TQ = 256
CH = 256
SHIFTS = (0, 1, 3, 2)
SLOT = {t: i for i, t in enumerate(SHIFTS)}


class Copies:
    def __init__(self, send_sems, recv_sems):
        self.send_sems, self.recv_sems, self.count, self.all = send_sems, recv_sems, 0, []

    def one(self, src, dst, send, recv, device):
        return pltpu.make_async_remote_copy(
            src_ref=src,
            dst_ref=dst,
            send_sem=self.send_sems.at[send],
            recv_sem=self.recv_sems.at[recv],
            device_id=device,
            device_id_type=pl.DeviceIdType.MESH,
        )

    def make(self, src, dst, **device):
        copy = self.one(src, dst, self.count, self.count, device)
        self.count += 1
        self.all.append(copy)
        return copy


class Heads:
    def __init__(self, d, dv, rows, groups, ins, refs, kv_pair, shared, copies):
        self.d, self.dv, self.rows, self.half, self.groups = d, dv, rows, rows // 2, groups
        self.q_in, self.k_in, self.v_in = ins
        self.q_s, self.kv_s, self.qt_s, self.vt_s, self.acc, self.m_s, self.l_s, self.st, self.st_in, self.part, self.part_in, self.relay, self.heads, self.out = refs
        self.kv = kv_pair
        self.tab, self.pos, self.s_a, self.s_b, self.t_a, self.t_b, self.p_scr = shared
        self.scale = d ** (-0.5) * LOG2E
        self.copies = copies
        z, x = lax.axis_index("z"), lax.axis_index("x")
        up = {"z": (z + 1) % 4}, {"z": (z + 3) % 4}
        right = {"x": (x + 1) % 4}, {"x": (x + 3) % 4}
        half = self.half
        one, three, two = SLOT[1], SLOT[3], SLOT[2]
        h0, h1 = pl.ds(0, half), pl.ds(half, half)
        lanes = (self.k_in, pl.ds(0, 2 * d)), (self.v_in, pl.ds(2 * d, dv))
        self.q_near = [copies.make(self.q_in, self.q_s.at[one], **up[0]), copies.make(self.q_in, self.q_s.at[three], **up[1])]
        self.q_far = [
            copies.make(self.q_s.at[one, h0], self.q_s.at[two, h0], **up[0]),
            copies.make(self.q_s.at[three, h1], self.q_s.at[two, h1], **up[1]),
        ]
        self.swap = [copies.make(src.at[h1], self.kv_at(1, 0, slice(None), at), z=3 - z) for src, at in lanes]
        self.own = [(src.at[h0], self.kv_at(0, 0, slice(None), at)) for src, at in lanes] + [(self.q_in, self.q_s.at[0])]
        quarter = half // 2
        g0, g1 = pl.ds(0, quarter), pl.ds(quarter, quarter)
        self.kv_near = [
            [[copies.make(src.at[h0], self.kv_at(0, slot, slice(None), at), **to) for src, at in lanes] for slot, to in ((one, right[0]), (three, right[1]))],
            [[copies.make(self.kv_at(1, 0), self.kv_at(1, slot), **to)] for slot, to in ((one, right[0]), (three, right[1]))],
        ]
        self.kv_far = [[
            copies.make(self.kv_at(b, one, g0), self.kv_at(b, two, g0), **right[0]),
            copies.make(self.kv_at(b, three, g1), self.kv_at(b, two, g1), **right[1]),
        ] for b in range(2)]
        self.st_out, self.part_near, self.part_first, self.part_far = [], [], [], []
        for p0, p1 in groups:
            cols = pl.ds(p0 * 4 * TQ, (p1 - p0) * 4 * TQ)
            self.st_out.append([copies.make(self.st.at[:, cols], self.st_in.at[t - 1, :, cols], z=(z + t) % 4) for t in (1, 2, 3)])
            size = (p1 - p0) * TQ
            all_, f0, f1 = pl.ds(p0 * TQ, size), pl.ds(p0 * TQ, size // 2), pl.ds(p0 * TQ + size // 2, size // 2)
            held = pl.ds(p0 * TQ // 2, size // 2)
            self.part_near.append([
                copies.make(self.part.at[one, all_], self.part_in.at[0, all_], **up[1]),
                copies.make(self.part.at[three, all_], self.part_in.at[1, all_], **up[0]),
            ])
            self.part_first.append([
                copies.make(self.part.at[two, f0], self.relay.at[0, held], **up[0]),
                copies.make(self.part.at[two, f1], self.relay.at[1, held], **up[1]),
            ])
            self.part_far.append([
                copies.make(self.relay.at[0, held], self.part_in.at[2, f0], **up[0]),
                copies.make(self.relay.at[1, held], self.part_in.at[2, f1], **up[1]),
            ])
        self.rank = lax.axis_index("y") * 2 + lax.axis_index("c")
        self.base = copies.count
        copies.count += 8

    def kv_at(self, b, *index):
        ref = self.kv[b] if self.kv else self.kv_s
        index = index if self.kv else (b,) + index
        return ref.at[index] if index else ref

    def to_token(self, r):
        mine = self.rows // 8
        at = pl.multiple_of(self.rank * self.dv, self.dv)
        return self.copies.one(
            self.heads.at[pl.ds(r * mine, mine)], self.out.at[:, pl.ds(at, self.dv)],
            self.base + r, self.base + self.rank, {"y": r // 2, "c": r % 2},
        )

    def from_rank(self, r):
        mine = self.rows // 8
        return self.copies.one(
            self.heads.at[pl.ds(r * mine, mine)], self.out.at[:, r * self.dv:(r + 1) * self.dv],
            self.base + r, self.base + r, {"y": r // 2, "c": r % 2},
        )

    def send_swap(self):
        for c in self.swap:
            c.start()

    def send_near(self):
        for c in self.kv_near[0][0] + self.kv_near[0][1] + self.q_near:
            c.start()

    def pass_swap(self):
        for c in self.swap:
            c.wait_recv()
        for near in self.kv_near[1]:
            near[0].start()

    def relay_queries(self):
        for near, far in zip(self.q_near, self.q_far):
            near.wait_recv()
            far.start()

    def relay_keys(self, b):
        for near, far in zip(self.kv_near[b], self.kv_far[b]):
            for c in near:
                c.wait_recv()
            far.start()

    def clear(self):
        self.m_s[...] = jnp.full_like(self.m_s, NEG)
        self.l_s[...] = jnp.zeros_like(self.l_s)

        def tile(n, _):
            self.acc[:, :, pl.ds(pl.multiple_of(n * TQ, TQ), TQ)] = jnp.zeros((2, self.dv, TQ), jnp.float32)
            return 0
        lax.fori_loop(0, 4 * self.rows // TQ, tile, 0)

    def turn_queries(self):
        for c in self.q_far:
            c.wait_recv()

        def turn(i, _):
            for p in range(self.rows // TQ):
                at = pl.multiple_of((p * 4 + i) * TQ, TQ)
                self.qt_s[:, pl.ds(at, TQ)] = self.q_s[i, p * TQ:(p + 1) * TQ].T
            return 0
        lax.fori_loop(0, 4, turn, 0)

    def wait_values(self, b):
        for c in self.kv_far[b]:
            c.wait_recv()

    def turn_values(self, b):
        d, dv, half = self.d, self.dv, self.half

        def turn(i, _):
            at = pl.multiple_of((b * 4 + i) * half, half)
            self.vt_s[:, pl.ds(at, half)] = self.kv_at(b)[i, :, 2 * d:2 * d + dv].T
            return 0
        lax.fori_loop(0, 4, turn, 0)

    def read(self, i, s_buf, t_buf, b=None):
        d, half = self.d, self.half
        q0 = pl.multiple_of(self.tab[0, i] * TQ, TQ)
        kj = self.tab[1, i]
        part, first = kj // 2, (kj % 2) * 2
        for w in range(2):
            qt = self.qt_s[w * d:(w + 1) * d, pl.ds(q0, TQ)]
            top = None
            for c in range(2):
                lanes = slice(w * d, (w + 1) * d)
                k = self.kv_s[part, first + c, :, lanes] if b is None else self.kv[b][first + c, :, lanes]
                s = jnp.dot(k, qt, preferred_element_type=jnp.float32)
                s_buf[w, c * half:(c + 1) * half] = s
                m8 = jnp.max(s.reshape(half // 8, 8, TQ), axis=0)
                top = m8 if top is None else jnp.maximum(top, m8)
            t_buf[w] = top

    def mask(self, i, s_buf, t_buf):
        rows, half = self.rows, self.half
        qi, kj = self.tab[0, i], self.tab[1, i]
        qp = self.pos[qi % 4] + (qi // 4) * TQ
        CM = 128
        t_buf[...] = jnp.full_like(t_buf, NEG)

        def chunk(c, _):
            r = pl.multiple_of(c * CM, CM)
            late = c // (half // CM)
            k0 = self.pos[4 + 2 * kj + late] + (c - late * (half // CM)) * CM
            keep = lax.broadcasted_iota(jnp.int32, (CM, TQ), 0) - lax.broadcasted_iota(jnp.int32, (CM, TQ), 1) <= qp - k0
            for w in range(2):
                s = jnp.where(keep, s_buf[w, pl.ds(r, CM)], NEG)
                s_buf[w, pl.ds(r, CM)] = s
                t_buf[w] = jnp.maximum(t_buf[w], jnp.max(s.reshape(CM // 8, 8, TQ), axis=0))
            return 0
        lax.fori_loop(0, rows // CM, chunk, 0)

    def weigh(self, i, s_buf, t_buf):
        rows = self.rows
        cols = pl.ds(pl.multiple_of(self.tab[0, i] * TQ, TQ), TQ)
        k0 = pl.multiple_of(self.tab[1, i] * rows, rows)
        for w in range(2):
            old = self.m_s[w:w + 1, cols]
            new = jnp.maximum(old, jnp.max(t_buf[w], axis=0, keepdims=True) * self.scale)
            f = jnp.exp2(old - new)
            self.m_s[w:w + 1, cols] = new
            tot = None
            for c in range(rows // CH):
                p = jnp.exp2(s_buf[w, c * CH:(c + 1) * CH] * self.scale - new)
                t8 = jnp.sum(p.reshape(CH // 8, 8, TQ), axis=0)
                tot = t8 if tot is None else tot + t8
                self.p_scr[w, c * CH:(c + 1) * CH] = p.astype(jnp.bfloat16)
            o = jnp.dot(self.vt_s[:, pl.ds(k0, rows)], self.p_scr[w], preferred_element_type=jnp.float32)
            self.l_s[w, :, cols] = self.l_s[w, :, cols] * f + tot
            self.acc[w, :, cols] = self.acc[w, :, cols] * f + o

    def run(self, low, high, hooks, b=None):
        def advance(i, cur, nxt):
            @pl.when(self.tab[2, i] == 1)
            def _():
                self.mask(i, *cur)
            self.read(jnp.minimum(i + 1, high - 1), *nxt, b)
            self.weigh(i, *cur)

        one, two = (self.s_a, self.t_a), (self.s_b, self.t_b)
        self.read(low, *one, b)
        turns = jnp.maximum((high - low + 1) // 2, len(hooks) + 1)

        def pair(n, _):
            for k, hook in enumerate(hooks):
                pl.when(n == turns * (k + 1) // (len(hooks) + 1))(hook)
            i = low + 2 * n

            @pl.when(i < high)
            def _():
                advance(i, one, two)

            @pl.when(i + 1 < high)
            def _():
                advance(i + 1, two, one)
            return 0
        lax.fori_loop(0, turns, pair, 0)

    def mix(self, g, slot, lam):
        dv = self.dv
        for p in range(*self.groups[g]):
            c0 = (p * 4 + slot) * TQ
            stats = [self.st[:, c0:c0 + TQ]]
            for t in (1, 2, 3):
                at = (p * 4 + SLOT[(SHIFTS[slot] - t) % 4]) * TQ
                stats.append(self.st_in[t - 1, :, at:at + TQ])
            weights = []
            for w in range(2):
                peaks = [s[w:w + 1] for s in stats]
                top = functools.reduce(jnp.maximum, peaks)
                total = sum(s[2 + w:3 + w] * jnp.exp2(m - top) for m, s in zip(peaks, stats))
                weights.append(jnp.exp2(peaks[0] - top) / total)
            mixed = self.acc[0, :, c0:c0 + TQ] * weights[0] - self.acc[1, :, c0:c0 + TQ] * (weights[1] * lam)
            self.part[slot, p * TQ:(p + 1) * TQ] = mixed.T.astype(jnp.bfloat16)

    def send_stats(self, g):
        p0, p1 = self.groups[g]
        cols = slice(p0 * 4 * TQ, p1 * 4 * TQ)
        self.st[0:2, cols] = self.m_s[:, cols]
        for w in range(2):
            self.st[2 + w:3 + w, cols] = jnp.sum(self.l_s[w, :, cols], axis=0, keepdims=True)
        for c in self.st_out[g]:
            c.start()

    def mix_and_send(self, g, lam):
        for c in self.st_out[g]:
            c.wait_recv()
        self.mix(g, SLOT[2], lam)
        for c in self.part_first[g]:
            c.start()
        self.mix(g, SLOT[1], lam)
        self.part_near[g][0].start()
        self.mix(g, SLOT[3], lam)
        self.part_near[g][1].start()

    def pass_parts(self, g):
        for first, far in zip(self.part_first[g], self.part_far[g]):
            first.wait_recv()
            far.start()

    def finish(self, g, lam):
        self.mix(g, 0, lam)
        for c in self.part_near[g] + self.part_far[g]:
            c.wait_recv()
        B = 128
        p0, p1 = self.groups[g]
        for at in range(p0 * TQ, p1 * TQ, B):
            r = slice(at, at + B)
            total = self.part[0, r].astype(jnp.float32)
            for n in range(3):
                total = total + self.part_in[n, r].astype(jnp.float32)
            total = total * lax.rsqrt(jnp.mean(total * total, axis=-1, keepdims=True) + 1e-06)
            self.heads[r] = total.astype(jnp.bfloat16)
        mine = self.rows // 8
        for r in range(8):
            if p0 * TQ < (r + 1) * mine <= p1 * TQ:
                pl.when(r != self.rank)(self.to_token(r).start)


class Weights:
    def __init__(self, ins, sizes, held, copies):
        self.held = held
        y, c = lax.axis_index("y"), lax.axis_index("c")
        up, down, pair = {"y": (y + 1) % 4}, {"y": (y + 3) % 4}, {"c": 1 - c}
        self.own, self.first, self.near, self.far, self.pass_near, self.pass_far = [], [], [], [], [], []
        base = 0
        for src, size in zip(ins, sizes):
            half = size // 2

            def rows(t, at=0, n=size, base=base, size=size):
                return held.at[pl.ds(pl.multiple_of(base + (((y + t) % 4) * 2 + c) * size + at, half), n)]
            self.own.append((src, rows(0)))
            self.first.append(copies.make(src, rows(0), **pair))
            self.near.append([copies.make(src, rows(0), **up), copies.make(src, rows(0), **down)])
            self.far.append([
                copies.make(rows(3, 0, half), rows(3, 0, half), **up),
                copies.make(rows(1, half, half), rows(1, half, half), **down),
            ])
            self.pass_near.append([copies.make(rows(3), rows(3), **pair), copies.make(rows(1), rows(1), **pair)])
            self.pass_far.append([copies.make(rows(2, 0, half), rows(2, 0, half), **pair), copies.make(rows(2, half, half), rows(2, half, half), **pair)])
            base += 8 * size

    def send(self):
        for near, first in zip(self.near, self.first):
            for c in near:
                c.start()
            first.start()

    def relay(self):
        for near, far, onward in zip(self.near, self.far, self.pass_near):
            for n, f, o in zip(near, far, onward):
                n.wait_recv()
                f.start()
                o.start()

    def last(self):
        for far, onward in zip(self.far, self.pass_far):
            for f, o in zip(far, onward):
                f.wait_recv()
                o.start()

    def wait(self):
        for c in self.first:
            c.wait_recv()
        for group in self.pass_near + self.pass_far:
            for c in group:
                c.wait_recv()


def attention_kernel(lam_ref, residual_ref, gain_ref, ow_in, on_in, qn_in, kn_in, vn_in, qw_in, kw_in, vw_in, stream_ref, normed_ref, *scratch, rows):
    narrow_refs, wide_refs = scratch[:14], scratch[14:28]
    shared, (send_sems, recv_sems, local_sems, weights_s, sum_s) = scratch[28:35], scratch[35:40]
    z, x = lax.axis_index("z"), lax.axis_index("x")
    half = rows // 2
    per = rows // TQ
    copies = Copies(send_sems, recv_sems)
    narrow = Heads(64, 128, rows, ((0, per - 1), (per - 1, per)), (qn_in, kn_in, vn_in), narrow_refs, None, shared, copies)
    wide = Heads(128, 256, rows, ((0, per),), (qw_in, kw_in, vw_in), wide_refs, scratch[40:42], shared, copies)
    weights = Weights((ow_in, on_in), (256, 128), weights_s, copies)
    lam_w, lam_n = lam_ref[0], lam_ref[1]

    barrier = pltpu.get_barrier_semaphore()
    for t in (1, 2, 3):
        pl.semaphore_signal(barrier, inc=1, device_id={"z": (z + t) % 4}, device_id_type=pl.DeviceIdType.MESH)
        pl.semaphore_signal(barrier, inc=1, device_id={"x": (x + t) % 4}, device_id_type=pl.DeviceIdType.MESH)
    rank = narrow.rank
    for k in range(1, 8):
        r = (rank + k) % 8
        pl.semaphore_signal(barrier, inc=1, device_id={"y": r // 2, "c": r % 2}, device_id_type=pl.DeviceIdType.MESH)
    local = []
    for h in (narrow, wide):
        for src, dst in h.own:
            local.append(pltpu.make_async_copy(src, dst, local_sems.at[len(local)]))
    for src, dst in weights.own:
        local.append(pltpu.make_async_copy(src, dst, local_sems.at[len(local)]))
    for c in local:
        c.start()
    pl.semaphore_wait(barrier, 13)

    wide.send_swap()
    wide.send_near()
    narrow.send_swap()
    weights.send()
    wide.clear()

    pos, tab = narrow.pos, narrow.tab
    for i, t in enumerate(SHIFTS):
        pos[i] = (4 * ((z + 4 - t) % 4) + x) * rows
        n = (x + 4 - t) % 4
        pos[4 + i] = (4 * z + n) * rows
        pos[8 + i] = (4 * (3 - z) + n) * rows + half

    def list_steps(p0, p1, k0, k1, n):
        def list_q(j, n):
            qi = 4 * p0 + j
            qp = pos[qi % 4] + (qi // 4) * TQ

            def list_k(kj, n):
                first, second = pos[4 + 2 * kj], pos[5 + 2 * kj]
                hi, lo = jnp.maximum(first, second), jnp.minimum(first, second)
                tab[0, n] = qi
                tab[1, n] = kj
                tab[2, n] = jnp.where(hi + half - 1 <= qp, 0, 1)
                return n + jnp.where(lo <= qp + TQ - 1, 1, 0)
            return lax.fori_loop(k0, k1, list_k, n)
        return lax.fori_loop(0, 4 * (p1 - p0), list_q, n)
    wide_a = list_steps(0, per, 0, 2, 0)
    wide_b = list_steps(0, per, 2, 4, wide_a)
    narrow_a = list_steps(0, per - 1, 0, 4, wide_b)
    narrow_b = list_steps(per - 1, per, 0, 4, narrow_a)
    for n in range(3):
        tab[n, narrow_b] = 0

    for c in local:
        c.wait()
    wide.relay_keys(0)
    wide.relay_queries()
    wide.pass_swap()
    narrow.send_near()
    narrow.clear()
    wide.turn_queries()
    wide.wait_values(0)
    wide.turn_values(0)

    def narrow_relays():
        narrow.relay_queries()
        narrow.relay_keys(0)
    wide.run(0, wide_a, [narrow.pass_swap, lambda: wide.relay_keys(1)], 0)
    wide.wait_values(1)
    wide.turn_values(1)
    wide.run(wide_a, wide_b, [narrow_relays, lambda: narrow.relay_keys(1)], 1)
    wide.send_stats(0)
    for b in range(2):
        narrow.wait_values(b)
    narrow.turn_queries()
    narrow.turn_values(0)
    narrow.turn_values(1)
    narrow.run(wide_b, narrow_a, [lambda: wide.mix_and_send(0, lam_w), weights.relay, lambda: wide.pass_parts(0)])
    narrow.send_stats(0)
    narrow.run(narrow_a, narrow_b, [lambda: narrow.mix_and_send(0, lam_n)])
    narrow.send_stats(1)
    wide.finish(0, lam_w)
    narrow.pass_parts(0)
    narrow.mix_and_send(1, lam_n)
    weights.last()
    narrow.finish(0, lam_n)
    narrow.pass_parts(1)
    mine = rows // 8
    width = weights_s.shape[1]

    def collect(h):
        for r in range(8):
            pl.when(r != rank)(h.from_rank(r).wait_recv)
        at = pl.multiple_of(rank * mine, mine)
        h.out[:, pl.ds(pl.multiple_of(rank * h.dv, h.dv), h.dv)] = h.heads[pl.ds(at, mine)]
    weights.wait()
    collect(wide)
    edge = 8 * wide.dv

    def project_wide(n, _):
        at = pl.ds(pl.multiple_of(n * 512, 512), 512)
        sum_s[:, at] = jnp.dot(wide.out[...], weights_s[0:edge, at], preferred_element_type=jnp.float32)
        return 0
    lax.fori_loop(0, width // 512, project_wide, 0)
    narrow.finish(1, lam_n)
    collect(narrow)

    def project(n, square):
        at = pl.ds(pl.multiple_of(n * 512, 512), 512)
        total = sum_s[:, at] + jnp.dot(narrow.out[...], weights_s[edge:, at], preferred_element_type=jnp.float32)
        stream = (total + residual_ref[:, at].astype(jnp.float32)).astype(jnp.bfloat16)
        stream_ref[:, at] = stream
        stream = stream.astype(jnp.float32)
        return square + jnp.sum(stream * stream, axis=-1, keepdims=True)
    square = lax.fori_loop(0, width // 512, project, jnp.zeros((mine, 1), jnp.float32))
    factor = lax.rsqrt(square / width + 1e-06)

    def norm(n, _):
        at = pl.ds(pl.multiple_of(n * 512, 512), 512)
        normed_ref[:, at] = (stream_ref[:, at].astype(jnp.float32) * factor * gain_ref[:, at]).astype(jnp.bfloat16)
        return 0
    lax.fori_loop(0, width // 512, norm, 0)
    for h in (narrow, wide):
        for r in range(8):
            pl.when(r != rank)(h.to_token(r).wait_send)
    for c in copies.all:
        c.wait_send()


def attention(qw, kw, vw, qn, kn, vn, lam, residual, out_w, out_n, gain):
    qw, kw, vw, qn, kn, vn = (a[:, 0] for a in (qw, kw, vw, qn, kn, vn))
    rows = qw.shape[0]
    half, mine = rows // 2, rows // 8
    total = 4 * rows
    bf16, f32 = jnp.bfloat16, jnp.float32

    def scratch(d, dv, both):
        return [
            pltpu.VMEM((4, rows, 2 * d), bf16),
            pltpu.VMEM((2, 4, half, 2 * d + dv) if both else (16, 128), bf16),
            pltpu.VMEM((2 * d, total), bf16),
            pltpu.VMEM((dv, total), bf16),
            pltpu.VMEM((2, dv, total), f32),
            pltpu.VMEM((2, total), f32),
            pltpu.VMEM((2, 8, total), f32),
            pltpu.VMEM((4, total), f32),
            pltpu.VMEM((3, 4, total), f32),
            pltpu.VMEM((4, rows, dv), bf16),
            pltpu.VMEM((3, rows, dv), bf16),
            pltpu.VMEM((2, half, dv), bf16),
            pltpu.VMEM((rows, dv), bf16),
            pltpu.VMEM((mine, 8 * dv), bf16),
        ]
    any_ = pl.BlockSpec(memory_space=pl.ANY)
    vmem = pl.BlockSpec(memory_space=pltpu.VMEM)
    count = 2 * (4 + 2 + 4 + 2 + 4 + 8) + 3 * 9 + 2 * 9
    width = residual.shape[1]
    return pl.pallas_call(
        functools.partial(attention_kernel, rows=rows),
        out_shape=(jax.ShapeDtypeStruct((mine, width), bf16),) * 2,
        in_specs=[pl.BlockSpec(memory_space=pltpu.SMEM), vmem, vmem] + [any_] * 8,
        out_specs=(vmem, vmem),
        scratch_shapes=scratch(64, 128, True) + scratch(128, 256, False) + [
            pltpu.SMEM((3, 2 * 4 * (rows // TQ) * 4 + 1), jnp.int32),
            pltpu.SMEM((12,), jnp.int32),
            pltpu.VMEM((2, rows, TQ), f32),
            pltpu.VMEM((2, rows, TQ), f32),
            pltpu.VMEM((2, 8, TQ), f32),
            pltpu.VMEM((2, 8, TQ), f32),
            pltpu.VMEM((2, rows, TQ), bf16),
            pltpu.SemaphoreType.DMA((count,)),
            pltpu.SemaphoreType.DMA((count,)),
            pltpu.SemaphoreType.DMA((8,)),
            pltpu.VMEM((8 * 384, width), bf16),
            pltpu.VMEM((mine, width), f32),
            pltpu.VMEM((4, half, 512), bf16),
            pltpu.VMEM((4, half, 512), bf16),
        ],
        name="attention",
        cost_estimate=pl.CostEstimate(flops=100 * 10**9, bytes_accessed=10**7, transcendentals=0),
        compiler_params=pltpu.CompilerParams(collective_id=0, has_side_effects=True, vmem_limit_bytes=60 * 2**20),
    )(lam.reshape(-1), residual, gain.reshape(1, -1), out_w, out_n, qn, kn, vn, qw, kw, vw)


def device_of(e):
    return {"z": e // 32, "x": (e // 8) % 4, "y": (e // 2) % 4, "c": e % 2}


def swapped(perm, rows):
    return jnp.dot(perm, rows, preferred_element_type=jnp.float32).astype(jnp.bfloat16)


def to_tiles(perm, block):
    width = block.shape[1] // 16
    stacked = jnp.concatenate([block[:, g * width:(g + 1) * width] for g in range(16)], axis=0)
    return swapped(perm, stacked).reshape(16, 16, width)


def experts_kernel(token_ref, slot_ref, weight_ref, normed_ref, stream_ref, gate_in, up_in, down_in, out_ref,
                   gate_s, up_s, down_s, perm_s, rows_s, stream_s, send_s, got_a, got_b, flat_s, hidden_s, ret_a, ret_b, back_s,
                   weight_sems, send_sems, recv_sems):
    count = 128
    cap = send_s.shape[0] // count
    total = send_s.shape[0]
    part = total // 2
    tokens = normed_ref.shape[0]
    me = ((lax.axis_index("z") * 4 + lax.axis_index("x")) * 4 + lax.axis_index("y")) * 2 + lax.axis_index("c")
    chip, core = me // 2, me % 2
    got, ret = (got_a, got_b), (ret_a, ret_b)
    loads = [
        pltpu.make_async_copy(src.at[0], dst, weight_sems.at[n])
        for n, (src, dst) in enumerate(((gate_in, gate_s), (up_in, up_s), (down_in, down_s)))
    ]
    for c in loads:
        c.start()
    barrier = pltpu.get_barrier_semaphore()

    def greet(k, _):
        pl.semaphore_signal(barrier, inc=1, device_id=device_of((me + k) % count), device_id_type=pl.DeviceIdType.MESH)
        return 0
    lax.fori_loop(1, count, greet, 0)

    r = lax.broadcasted_iota(jnp.int32, (256, 256), 0)
    c = lax.broadcasted_iota(jnp.int32, (256, 256), 1)
    perm_s[...] = jnp.where((r % 16) * 16 + r // 16 == c, 1.0, 0.0).astype(jnp.bfloat16)
    perm = perm_s[...]
    for b in range(tokens // 16):
        s = slice(b * 16, (b + 1) * 16)
        rows_s[s] = to_tiles(perm, normed_ref[s])

    def fill(n, _):
        for u in range(8):
            send_s[n * 8 + u] = rows_s[token_ref[n * 8 + u]]
        return 0
    lax.fori_loop(0, total // 8, fill, 0)
    pl.semaphore_wait(barrier, count - 1)

    def peer(h, j):
        other = (chip + j) % 64
        return other, other * 2 + (core if h == 0 else 1 - core)

    def remote(src, dst, way, n, e):
        return pltpu.make_async_remote_copy(
            src_ref=src, dst_ref=dst, send_sem=send_sems.at[way, n], recv_sem=recv_sems.at[way, n],
            device_id=device_of(e), device_id_type=pl.DeviceIdType.MESH,
        )

    def there(h, j):
        _, e = peer(h, j)
        return remote(send_s.at[pl.ds(e * cap, cap)], got[h].at[pl.ds(chip * cap, cap)], 0, h * 64 + j, e)

    def back(h, j):
        other, e = peer(h, j)
        return remote(ret[h].at[pl.ds(other * cap, cap)], back_s.at[pl.ds(me * cap, cap)], 1, h * 64 + j, e)

    def each(h, act):
        def go(n, _):
            act(h, (n * 27) % 64)
            return 0
        lax.fori_loop(1 - h, 64, go, 0)

    each(0, lambda h, j: there(h, j).start())
    got_a[pl.ds(chip * cap, cap)] = send_s[pl.ds(me * cap, cap)]
    each(1, lambda h, j: there(h, j).start())
    for b in range(tokens // 16):
        s = slice(b * 16, (b + 1) * 16)
        stream_s[s] = to_tiles(perm, stream_ref[s])
    for c in loads:
        c.wait()

    for h in range(2):
        each(h, lambda h, j: there(h, j).wait_recv())

        def flatten(n, _):
            for u in range(4):
                at = pl.multiple_of((n * 4 + u) * 16, 16)
                turned = swapped(perm, got[h][pl.ds(at, 16)].reshape(256, 128))
                for g in range(16):
                    flat_s[pl.ds(at, 16), g * 128:(g + 1) * 128] = turned[g * 16:(g + 1) * 16]
            return 0
        lax.fori_loop(0, part // 64, flatten, 0)

        def first(n, _):
            at = pl.ds(pl.multiple_of(n * 256, 256), 256)
            gate = jnp.dot(flat_s[...], gate_s[:, at], preferred_element_type=jnp.float32)
            up = jnp.dot(flat_s[...], up_s[:, at], preferred_element_type=jnp.float32)
            hidden_s[:, at] = (gate * jax.nn.sigmoid(gate) * up).astype(jnp.bfloat16)
            return 0
        lax.fori_loop(0, hidden_s.shape[1] // 256, first, 0)

        def second(n, _):
            at = pl.ds(pl.multiple_of(n * 256, 256), 256)
            flat_s[:, at] = jnp.dot(hidden_s[...], down_s[:, at], preferred_element_type=jnp.float32).astype(jnp.bfloat16)
            return 0
        lax.fori_loop(0, flat_s.shape[1] // 256, second, 0)

        def unflatten(n, _):
            for u in range(4):
                at = pl.ds(pl.multiple_of((n * 4 + u) * 16, 16), 16)
                ret[h][at] = to_tiles(perm, flat_s[at, :])
            return 0
        lax.fori_loop(0, part // 64, unflatten, 0)
        each(h, lambda h, j: back(h, j).start())
    back_s[pl.ds(me * cap, cap)] = ret_a[pl.ds(chip * cap, cap)]
    for h in range(2):
        each(h, lambda h, j: back(h, j).wait_recv())

    def combine(n, _):
        for u in range(4):
            t = n * 4 + u
            summed = weight_ref[2 * t] * back_s[slot_ref[2 * t]].astype(jnp.float32)
            summed = summed + weight_ref[2 * t + 1] * back_s[slot_ref[2 * t + 1]].astype(jnp.float32)
            rows_s[t] = (stream_s[t].astype(jnp.float32) + summed).astype(jnp.bfloat16)
        return 0
    lax.fori_loop(0, tokens // 4, combine, 0)
    for b in range(tokens // 16):
        s = slice(b * 16, (b + 1) * 16)
        turned = swapped(perm, rows_s[s].reshape(256, 128))
        for g in range(16):
            out_ref[s, g * 128:(g + 1) * 128] = turned[g * 16:(g + 1) * 16]
    for h in range(2):
        each(h, lambda h, j: there(h, j).wait_send())
        each(h, lambda h, j: back(h, j).wait_send())


def experts(token_of_slot, slot_of_token, weight, normed, stream, gate, up, down):
    tokens, width = normed.shape
    slots = token_of_slot.shape[0]
    inner = gate.shape[2]
    smem = pl.BlockSpec(memory_space=pltpu.SMEM)
    vmem = pl.BlockSpec(memory_space=pltpu.VMEM)
    any_ = pl.BlockSpec(memory_space=pl.ANY)
    bf16 = jnp.bfloat16
    return pl.pallas_call(
        experts_kernel,
        out_shape=jax.ShapeDtypeStruct((tokens, width), bf16),
        in_specs=[smem] * 3 + [vmem] * 2 + [any_] * 3,
        out_specs=vmem,
        scratch_shapes=[
            pltpu.VMEM((width, inner), bf16),
            pltpu.VMEM((width, inner), bf16),
            pltpu.VMEM((inner, width), bf16),
            pltpu.VMEM((256, 256), bf16),
            pltpu.VMEM((tokens, 16, width // 16), bf16),
            pltpu.VMEM((tokens, 16, width // 16), bf16),
            pltpu.VMEM((slots, 16, width // 16), bf16),
            pltpu.VMEM((slots // 2, 16, width // 16), bf16),
            pltpu.VMEM((slots // 2, 16, width // 16), bf16),
            pltpu.VMEM((slots // 2, width), bf16),
            pltpu.VMEM((slots // 2, inner), bf16),
            pltpu.VMEM((slots // 2, 16, width // 16), bf16),
            pltpu.VMEM((slots // 2, 16, width // 16), bf16),
            pltpu.VMEM((slots, 16, width // 16), bf16),
            pltpu.SemaphoreType.DMA((3,)),
            pltpu.SemaphoreType.DMA((2, 128)),
            pltpu.SemaphoreType.DMA((2, 128)),
        ],
        name="experts",
        cost_estimate=pl.CostEstimate(flops=50 * 10**9, bytes_accessed=2 * 10**7, transcendentals=0),
        compiler_params=pltpu.CompilerParams(collective_id=1, has_side_effects=True, vmem_limit_bytes=60 * 2**20),
    )(token_of_slot, slot_of_token, weight, normed, stream, gate, up, down)


def shards(
    query_wide,
    key_wide,
    value_wide,
    query_narrow,
    key_narrow,
    value_narrow,
    mix_lambda,
    residual_in,
    out_wide,
    out_narrow,
    ffn_gain,
    expert_ids,
    expert_weights,
    gate_weight,
    up_weight,
    down_weight,
):
    tok_count, local_heads, _ = query_wide.shape
    stream, normed = attention(
        query_wide, key_wide, value_wide, query_narrow, key_narrow, value_narrow, mix_lambda,
        residual_in, out_wide, out_narrow, ffn_gain,
    )
    tp_size = lax.axis_size(TP)
    local_rows = tok_count // tp_size
    experts_all = lax.axis_size(SP) * tp_size
    capacity = max(2, 4 * local_rows // experts_all)
    flat_expert = expert_ids.reshape(-1)
    expert_hot = (flat_expert[:, None] == jnp.arange(experts_all, dtype=jnp.int32)[None, :]).astype(
        jnp.int32
    )
    slot_rank = jnp.sum((jnp.cumsum(expert_hot, axis=0) - 1) * expert_hot, axis=1)
    flat_slot = flat_expert * capacity + slot_rank
    slot_ids = jnp.arange(experts_all * capacity, dtype=jnp.int32)
    placed = slot_ids[:, None] == flat_slot[None, :]
    token = jnp.arange(2 * local_rows, dtype=jnp.int32) // 2
    token_of_slot = jnp.max(jnp.where(placed, token[None, :], 0), axis=1)
    return experts(
        token_of_slot, flat_slot, expert_weights.reshape(-1), normed, stream, gate_weight, up_weight, down_weight
    )


def solution(mesh):
    finer = Mesh(mesh.devices.reshape(4, 4, 4, 2), ("z", "x", "y", "c"))
    placed = (
        P(SP, TP, None),
        P(SP, TP, None),
        P(SP, TP, None),
        P(SP, TP, None),
        P(SP, TP, None),
        P(SP, TP, None),
        P(None, TP),
        P(SP_TP, None),
        P(TP, None),
        P(TP, None),
        P(),
        P(SP_TP, None),
        P(SP_TP, None),
        P(SP_TP, None, None),
        P(SP_TP, None, None),
        P(SP_TP, None, None),
    )
    return jax.shard_map(
        shards, mesh=finer, in_specs=placed, out_specs=P(SP_TP, None), check_vma=False
    )
```

```python
import functools
import jax
import jax.numpy as jnp
from jax import lax
from jax.experimental import pallas as pl
from jax.experimental.pallas import tpu as pltpu
from jax.sharding import Mesh
from jax.sharding import PartitionSpec as P

TP = ("y", "c")
SP = ("z", "x")
SP_TP = ("z", "x", "y", "c")

NEG = -1e30
LOG2E = 1.4426950408889634
TQ = 256
CH = 256
SHIFTS = (0, 1, 3, 2)
SLOT = {t: i for i, t in enumerate(SHIFTS)}


class Copies:
    def __init__(self, send_sems, recv_sems):
        self.send_sems, self.recv_sems, self.count, self.all = send_sems, recv_sems, 0, []

    def one(self, src, dst, send, recv, device):
        return pltpu.make_async_remote_copy(
            src_ref=src,
            dst_ref=dst,
            send_sem=self.send_sems.at[send],
            recv_sem=self.recv_sems.at[recv],
            device_id=device,
            device_id_type=pl.DeviceIdType.MESH,
        )

    def make(self, src, dst, **device):
        copy = self.one(src, dst, self.count, self.count, device)
        self.count += 1
        self.all.append(copy)
        return copy


class Heads:
    def __init__(self, d, dv, rows, groups, ins, refs, kv_pair, shared, copies):
        self.d, self.dv, self.rows, self.half, self.groups = d, dv, rows, rows // 2, groups
        self.q_in, self.k_in, self.v_in = ins
        self.q_s, self.kv_s, self.qt_s, self.vt_s, self.acc, self.m_s, self.l_s, self.st, self.st_in, self.part, self.part_in, self.relay, self.heads, self.out = refs
        self.kv = kv_pair
        self.tab, self.pos, self.s_a, self.s_b, self.t_a, self.t_b, self.p_scr = shared
        self.scale = d ** (-0.5) * LOG2E
        self.copies = copies
        z, x = lax.axis_index("z"), lax.axis_index("x")
        up = {"z": (z + 1) % 4}, {"z": (z + 3) % 4}
        right = {"x": (x + 1) % 4}, {"x": (x + 3) % 4}
        half = self.half
        one, three, two = SLOT[1], SLOT[3], SLOT[2]
        h0, h1 = pl.ds(0, half), pl.ds(half, half)
        lanes = (self.k_in, pl.ds(0, 2 * d)), (self.v_in, pl.ds(2 * d, dv))
        self.q_near = [copies.make(self.q_in, self.q_s.at[one], **up[0]), copies.make(self.q_in, self.q_s.at[three], **up[1])]
        self.q_far = [
            copies.make(self.q_s.at[one, h0], self.q_s.at[two, h0], **up[0]),
            copies.make(self.q_s.at[three, h1], self.q_s.at[two, h1], **up[1]),
        ]
        self.swap = [copies.make(src.at[h1], self.kv_at(1, 0, slice(None), at), z=3 - z) for src, at in lanes]
        self.own = [(src.at[h0], self.kv_at(0, 0, slice(None), at)) for src, at in lanes] + [(self.q_in, self.q_s.at[0])]
        quarter = half // 2
        g0, g1 = pl.ds(0, quarter), pl.ds(quarter, quarter)
        self.kv_near = [
            [[copies.make(src.at[h0], self.kv_at(0, slot, slice(None), at), **to) for src, at in lanes] for slot, to in ((one, right[0]), (three, right[1]))],
            [[copies.make(self.kv_at(1, 0), self.kv_at(1, slot), **to)] for slot, to in ((one, right[0]), (three, right[1]))],
        ]
        self.kv_far = [[
            copies.make(self.kv_at(b, one, g0), self.kv_at(b, two, g0), **right[0]),
            copies.make(self.kv_at(b, three, g1), self.kv_at(b, two, g1), **right[1]),
        ] for b in range(2)]
        self.st_out, self.part_near, self.part_first, self.part_far = [], [], [], []
        for p0, p1 in groups:
            cols = pl.ds(p0 * 4 * TQ, (p1 - p0) * 4 * TQ)
            self.st_out.append([copies.make(self.st.at[:, cols], self.st_in.at[t - 1, :, cols], z=(z + t) % 4) for t in (1, 2, 3)])
            size = (p1 - p0) * TQ
            all_, f0, f1 = pl.ds(p0 * TQ, size), pl.ds(p0 * TQ, size // 2), pl.ds(p0 * TQ + size // 2, size // 2)
            held = pl.ds(p0 * TQ // 2, size // 2)
            self.part_near.append([
                copies.make(self.part.at[one, all_], self.part_in.at[0, all_], **up[1]),
                copies.make(self.part.at[three, all_], self.part_in.at[1, all_], **up[0]),
            ])
            self.part_first.append([
                copies.make(self.part.at[two, f0], self.relay.at[0, held], **up[0]),
                copies.make(self.part.at[two, f1], self.relay.at[1, held], **up[1]),
            ])
            self.part_far.append([
                copies.make(self.relay.at[0, held], self.part_in.at[2, f0], **up[0]),
                copies.make(self.relay.at[1, held], self.part_in.at[2, f1], **up[1]),
            ])
        self.rank = lax.axis_index("y") * 2 + lax.axis_index("c")
        self.base = copies.count
        copies.count += 8

    def kv_at(self, b, *index):
        ref = self.kv[b] if self.kv else self.kv_s
        index = index if self.kv else (b,) + index
        return ref.at[index] if index else ref

    def to_token(self, r):
        mine = self.rows // 8
        at = pl.multiple_of(self.rank * self.dv, self.dv)
        return self.copies.one(
            self.heads.at[pl.ds(r * mine, mine)], self.out.at[:, pl.ds(at, self.dv)],
            self.base + r, self.base + self.rank, {"y": r // 2, "c": r % 2},
        )

    def from_rank(self, r):
        mine = self.rows // 8
        return self.copies.one(
            self.heads.at[pl.ds(r * mine, mine)], self.out.at[:, r * self.dv:(r + 1) * self.dv],
            self.base + r, self.base + r, {"y": r // 2, "c": r % 2},
        )

    def send_swap(self):
        for c in self.swap:
            c.start()

    def send_near(self):
        for c in self.kv_near[0][0] + self.kv_near[0][1] + self.q_near:
            c.start()

    def pass_swap(self):
        for c in self.swap:
            c.wait_recv()
        for near in self.kv_near[1]:
            near[0].start()

    def relay_queries(self):
        for near, far in zip(self.q_near, self.q_far):
            near.wait_recv()
            far.start()

    def relay_keys(self, b):
        for near, far in zip(self.kv_near[b], self.kv_far[b]):
            for c in near:
                c.wait_recv()
            far.start()

    def clear(self):
        self.m_s[...] = jnp.full_like(self.m_s, NEG)
        self.l_s[...] = jnp.zeros_like(self.l_s)

        def tile(n, _):
            self.acc[:, :, pl.ds(pl.multiple_of(n * TQ, TQ), TQ)] = jnp.zeros((2, self.dv, TQ), jnp.float32)
            return 0
        lax.fori_loop(0, 4 * self.rows // TQ, tile, 0)

    def turn_queries(self):
        for c in self.q_far:
            c.wait_recv()

        def turn(i, _):
            for p in range(self.rows // TQ):
                at = pl.multiple_of((p * 4 + i) * TQ, TQ)
                self.qt_s[:, pl.ds(at, TQ)] = self.q_s[i, p * TQ:(p + 1) * TQ].T
            return 0
        lax.fori_loop(0, 4, turn, 0)

    def wait_values(self, b):
        for c in self.kv_far[b]:
            c.wait_recv()

    def turn_values(self, b):
        d, dv, half = self.d, self.dv, self.half

        def turn(i, _):
            at = pl.multiple_of((b * 4 + i) * half, half)
            self.vt_s[:, pl.ds(at, half)] = self.kv_at(b)[i, :, 2 * d:2 * d + dv].T
            return 0
        lax.fori_loop(0, 4, turn, 0)

    def read(self, i, s_buf, t_buf, b=None):
        d, half = self.d, self.half
        q0 = pl.multiple_of(self.tab[0, i] * TQ, TQ)
        kj = self.tab[1, i]
        part, first = kj // 2, (kj % 2) * 2
        for w in range(2):
            qt = self.qt_s[w * d:(w + 1) * d, pl.ds(q0, TQ)]
            top = None
            for c in range(2):
                lanes = slice(w * d, (w + 1) * d)
                k = self.kv_s[part, first + c, :, lanes] if b is None else self.kv[b][first + c, :, lanes]
                s = jnp.dot(k, qt, preferred_element_type=jnp.float32)
                s_buf[w, c * half:(c + 1) * half] = s
                m8 = jnp.max(s.reshape(half // 8, 8, TQ), axis=0)
                top = m8 if top is None else jnp.maximum(top, m8)
            t_buf[w] = top

    def mask(self, i, s_buf, t_buf):
        rows, half = self.rows, self.half
        qi, kj = self.tab[0, i], self.tab[1, i]
        qp = self.pos[qi % 4] + (qi // 4) * TQ
        CM = 128
        t_buf[...] = jnp.full_like(t_buf, NEG)

        def chunk(c, _):
            r = pl.multiple_of(c * CM, CM)
            late = c // (half // CM)
            k0 = self.pos[4 + 2 * kj + late] + (c - late * (half // CM)) * CM
            keep = lax.broadcasted_iota(jnp.int32, (CM, TQ), 0) - lax.broadcasted_iota(jnp.int32, (CM, TQ), 1) <= qp - k0
            for w in range(2):
                s = jnp.where(keep, s_buf[w, pl.ds(r, CM)], NEG)
                s_buf[w, pl.ds(r, CM)] = s
                t_buf[w] = jnp.maximum(t_buf[w], jnp.max(s.reshape(CM // 8, 8, TQ), axis=0))
            return 0
        lax.fori_loop(0, rows // CM, chunk, 0)

    def weigh(self, i, s_buf, t_buf):
        rows = self.rows
        cols = pl.ds(pl.multiple_of(self.tab[0, i] * TQ, TQ), TQ)
        k0 = pl.multiple_of(self.tab[1, i] * rows, rows)
        for w in range(2):
            old = self.m_s[w:w + 1, cols]
            new = jnp.maximum(old, jnp.max(t_buf[w], axis=0, keepdims=True) * self.scale)
            f = jnp.exp2(old - new)
            self.m_s[w:w + 1, cols] = new
            tot = None
            for c in range(rows // CH):
                p = jnp.exp2(s_buf[w, c * CH:(c + 1) * CH] * self.scale - new)
                t8 = jnp.sum(p.reshape(CH // 8, 8, TQ), axis=0)
                tot = t8 if tot is None else tot + t8
                self.p_scr[w, c * CH:(c + 1) * CH] = p.astype(jnp.bfloat16)
            o = jnp.dot(self.vt_s[:, pl.ds(k0, rows)], self.p_scr[w], preferred_element_type=jnp.float32)
            self.l_s[w, :, cols] = self.l_s[w, :, cols] * f + tot
            self.acc[w, :, cols] = self.acc[w, :, cols] * f + o

    def run(self, low, high, hooks, b=None):
        def advance(i, cur, nxt):
            @pl.when(self.tab[2, i] == 1)
            def _():
                self.mask(i, *cur)
            self.read(jnp.minimum(i + 1, high - 1), *nxt, b)
            self.weigh(i, *cur)

        one, two = (self.s_a, self.t_a), (self.s_b, self.t_b)
        self.read(low, *one, b)
        turns = jnp.maximum((high - low + 1) // 2, len(hooks) + 1)

        def pair(n, _):
            for k, hook in enumerate(hooks):
                pl.when(n == turns * (k + 1) // (len(hooks) + 1))(hook)
            i = low + 2 * n

            @pl.when(i < high)
            def _():
                advance(i, one, two)

            @pl.when(i + 1 < high)
            def _():
                advance(i + 1, two, one)
            return 0
        lax.fori_loop(0, turns, pair, 0)

    def mix(self, g, slot, lam):
        dv = self.dv
        for p in range(*self.groups[g]):
            c0 = (p * 4 + slot) * TQ
            stats = [self.st[:, c0:c0 + TQ]]
            for t in (1, 2, 3):
                at = (p * 4 + SLOT[(SHIFTS[slot] - t) % 4]) * TQ
                stats.append(self.st_in[t - 1, :, at:at + TQ])
            weights = []
            for w in range(2):
                peaks = [s[w:w + 1] for s in stats]
                top = functools.reduce(jnp.maximum, peaks)
                total = sum(s[2 + w:3 + w] * jnp.exp2(m - top) for m, s in zip(peaks, stats))
                weights.append(jnp.exp2(peaks[0] - top) / total)
            mixed = self.acc[0, :, c0:c0 + TQ] * weights[0] - self.acc[1, :, c0:c0 + TQ] * (weights[1] * lam)
            self.part[slot, p * TQ:(p + 1) * TQ] = mixed.T.astype(jnp.bfloat16)

    def send_stats(self, g):
        p0, p1 = self.groups[g]
        cols = slice(p0 * 4 * TQ, p1 * 4 * TQ)
        self.st[0:2, cols] = self.m_s[:, cols]
        for w in range(2):
            self.st[2 + w:3 + w, cols] = jnp.sum(self.l_s[w, :, cols], axis=0, keepdims=True)
        for c in self.st_out[g]:
            c.start()

    def mix_and_send(self, g, lam):
        for c in self.st_out[g]:
            c.wait_recv()
        self.mix(g, SLOT[2], lam)
        for c in self.part_first[g]:
            c.start()
        self.mix(g, SLOT[1], lam)
        self.part_near[g][0].start()
        self.mix(g, SLOT[3], lam)
        self.part_near[g][1].start()

    def pass_parts(self, g):
        for first, far in zip(self.part_first[g], self.part_far[g]):
            first.wait_recv()
            far.start()

    def finish(self, g, lam):
        self.mix(g, 0, lam)
        for c in self.part_near[g] + self.part_far[g]:
            c.wait_recv()
        B = 128
        p0, p1 = self.groups[g]
        for at in range(p0 * TQ, p1 * TQ, B):
            r = slice(at, at + B)
            total = self.part[0, r].astype(jnp.float32)
            for n in range(3):
                total = total + self.part_in[n, r].astype(jnp.float32)
            total = total * lax.rsqrt(jnp.mean(total * total, axis=-1, keepdims=True) + 1e-06)
            self.heads[r] = total.astype(jnp.bfloat16)
        mine = self.rows // 8
        for r in range(8):
            if p0 * TQ < (r + 1) * mine <= p1 * TQ:
                pl.when(r != self.rank)(self.to_token(r).start)


class Weights:
    def __init__(self, ins, sizes, held, copies):
        self.held = held
        y, c = lax.axis_index("y"), lax.axis_index("c")
        up, down, pair = {"y": (y + 1) % 4}, {"y": (y + 3) % 4}, {"c": 1 - c}
        self.own, self.first, self.near, self.far, self.pass_near, self.pass_far = [], [], [], [], [], []
        base = 0
        for src, size in zip(ins, sizes):
            half = size // 2

            def rows(t, at=0, n=size, base=base, size=size):
                return held.at[pl.ds(pl.multiple_of(base + (((y + t) % 4) * 2 + c) * size + at, half), n)]
            self.own.append((src, rows(0)))
            self.first.append(copies.make(src, rows(0), **pair))
            self.near.append([copies.make(src, rows(0), **up), copies.make(src, rows(0), **down)])
            self.far.append([
                copies.make(rows(3, 0, half), rows(3, 0, half), **up),
                copies.make(rows(1, half, half), rows(1, half, half), **down),
            ])
            self.pass_near.append([copies.make(rows(3), rows(3), **pair), copies.make(rows(1), rows(1), **pair)])
            self.pass_far.append([copies.make(rows(2, 0, half), rows(2, 0, half), **pair), copies.make(rows(2, half, half), rows(2, half, half), **pair)])
            base += 8 * size

    def send(self):
        for near, first in zip(self.near, self.first):
            for c in near:
                c.start()
            first.start()

    def relay(self):
        for near, far, onward in zip(self.near, self.far, self.pass_near):
            for n, f, o in zip(near, far, onward):
                n.wait_recv()
                f.start()
                o.start()

    def last(self):
        for far, onward in zip(self.far, self.pass_far):
            for f, o in zip(far, onward):
                f.wait_recv()
                o.start()

    def wait(self):
        for c in self.first:
            c.wait_recv()
        for group in self.pass_near + self.pass_far:
            for c in group:
                c.wait_recv()


def attention_kernel(lam_ref, residual_ref, gain_ref, ow_in, on_in, qn_in, kn_in, vn_in, qw_in, kw_in, vw_in, stream_ref, normed_ref, *scratch, rows):
    narrow_refs, wide_refs = scratch[:14], scratch[14:28]
    shared, (send_sems, recv_sems, local_sems, weights_s, sum_s) = scratch[28:35], scratch[35:40]
    z, x = lax.axis_index("z"), lax.axis_index("x")
    half = rows // 2
    per = rows // TQ
    copies = Copies(send_sems, recv_sems)
    narrow = Heads(64, 128, rows, ((0, per - 1), (per - 1, per)), (qn_in, kn_in, vn_in), narrow_refs, None, shared, copies)
    wide = Heads(128, 256, rows, ((0, per),), (qw_in, kw_in, vw_in), wide_refs, scratch[40:42], shared, copies)
    weights = Weights((ow_in, on_in), (256, 128), weights_s, copies)
    lam_w, lam_n = lam_ref[0], lam_ref[1]

    barrier = pltpu.get_barrier_semaphore()
    for t in (1, 2, 3):
        pl.semaphore_signal(barrier, inc=1, device_id={"z": (z + t) % 4}, device_id_type=pl.DeviceIdType.MESH)
        pl.semaphore_signal(barrier, inc=1, device_id={"x": (x + t) % 4}, device_id_type=pl.DeviceIdType.MESH)
    rank = narrow.rank
    for k in range(1, 8):
        r = (rank + k) % 8
        pl.semaphore_signal(barrier, inc=1, device_id={"y": r // 2, "c": r % 2}, device_id_type=pl.DeviceIdType.MESH)
    local = []
    for h in (narrow, wide):
        for src, dst in h.own:
            local.append(pltpu.make_async_copy(src, dst, local_sems.at[len(local)]))
    for src, dst in weights.own:
        local.append(pltpu.make_async_copy(src, dst, local_sems.at[len(local)]))
    for c in local:
        c.start()
    pl.semaphore_wait(barrier, 13)

    wide.send_swap()
    wide.send_near()
    narrow.send_swap()
    weights.send()
    wide.clear()

    pos, tab = narrow.pos, narrow.tab
    for i, t in enumerate(SHIFTS):
        pos[i] = (4 * ((z + 4 - t) % 4) + x) * rows
        n = (x + 4 - t) % 4
        pos[4 + i] = (4 * z + n) * rows
        pos[8 + i] = (4 * (3 - z) + n) * rows + half

    def list_steps(p0, p1, k0, k1, n):
        def list_q(j, n):
            qi = 4 * p0 + j
            qp = pos[qi % 4] + (qi // 4) * TQ

            def list_k(kj, n):
                first, second = pos[4 + 2 * kj], pos[5 + 2 * kj]
                hi, lo = jnp.maximum(first, second), jnp.minimum(first, second)
                tab[0, n] = qi
                tab[1, n] = kj
                tab[2, n] = jnp.where(hi + half - 1 <= qp, 0, 1)
                return n + jnp.where(lo <= qp + TQ - 1, 1, 0)
            return lax.fori_loop(k0, k1, list_k, n)
        return lax.fori_loop(0, 4 * (p1 - p0), list_q, n)
    wide_a = list_steps(0, per, 0, 2, 0)
    wide_b = list_steps(0, per, 2, 4, wide_a)
    narrow_a = list_steps(0, per - 1, 0, 4, wide_b)
    narrow_b = list_steps(per - 1, per, 0, 4, narrow_a)
    for n in range(3):
        tab[n, narrow_b] = 0

    for c in local:
        c.wait()
    wide.relay_keys(0)
    wide.relay_queries()
    wide.pass_swap()
    narrow.send_near()
    narrow.clear()
    wide.turn_queries()
    wide.wait_values(0)
    wide.turn_values(0)

    def narrow_relays():
        narrow.relay_queries()
        narrow.relay_keys(0)
    wide.run(0, wide_a, [narrow.pass_swap, lambda: wide.relay_keys(1)], 0)
    wide.wait_values(1)
    wide.turn_values(1)
    wide.run(wide_a, wide_b, [narrow_relays, lambda: narrow.relay_keys(1)], 1)
    wide.send_stats(0)
    for b in range(2):
        narrow.wait_values(b)
    narrow.turn_queries()
    narrow.turn_values(0)
    narrow.turn_values(1)
    narrow.run(wide_b, narrow_a, [lambda: wide.mix_and_send(0, lam_w), weights.relay, lambda: wide.pass_parts(0)])
    narrow.send_stats(0)
    narrow.run(narrow_a, narrow_b, [lambda: narrow.mix_and_send(0, lam_n)])
    narrow.send_stats(1)
    wide.finish(0, lam_w)
    narrow.pass_parts(0)
    narrow.mix_and_send(1, lam_n)
    weights.last()
    narrow.finish(0, lam_n)
    narrow.pass_parts(1)
    mine = rows // 8
    width = weights_s.shape[1]

    def collect(h):
        for r in range(8):
            pl.when(r != rank)(h.from_rank(r).wait_recv)
        at = pl.multiple_of(rank * mine, mine)
        h.out[:, pl.ds(pl.multiple_of(rank * h.dv, h.dv), h.dv)] = h.heads[pl.ds(at, mine)]
    weights.wait()
    collect(wide)
    edge = 8 * wide.dv

    def project_wide(n, _):
        at = pl.ds(pl.multiple_of(n * 512, 512), 512)
        sum_s[:, at] = jnp.dot(wide.out[...], weights_s[0:edge, at], preferred_element_type=jnp.float32)
        return 0
    lax.fori_loop(0, width // 512, project_wide, 0)
    narrow.finish(1, lam_n)
    collect(narrow)

    def project(n, square):
        at = pl.ds(pl.multiple_of(n * 512, 512), 512)
        total = sum_s[:, at] + jnp.dot(narrow.out[...], weights_s[edge:, at], preferred_element_type=jnp.float32)
        stream = (total + residual_ref[:, at].astype(jnp.float32)).astype(jnp.bfloat16)
        stream_ref[:, at] = stream
        stream = stream.astype(jnp.float32)
        return square + jnp.sum(stream * stream, axis=-1, keepdims=True)
    square = lax.fori_loop(0, width // 512, project, jnp.zeros((mine, 1), jnp.float32))
    factor = lax.rsqrt(square / width + 1e-06)

    def norm(n, _):
        at = pl.ds(pl.multiple_of(n * 512, 512), 512)
        normed_ref[:, at] = (stream_ref[:, at].astype(jnp.float32) * factor * gain_ref[:, at]).astype(jnp.bfloat16)
        return 0
    lax.fori_loop(0, width // 512, norm, 0)
    for h in (narrow, wide):
        for r in range(8):
            pl.when(r != rank)(h.to_token(r).wait_send)
    for c in copies.all:
        c.wait_send()


def attention(qw, kw, vw, qn, kn, vn, lam, residual, out_w, out_n, gain):
    qw, kw, vw, qn, kn, vn = (a[:, 0] for a in (qw, kw, vw, qn, kn, vn))
    rows = qw.shape[0]
    half, mine = rows // 2, rows // 8
    total = 4 * rows
    bf16, f32 = jnp.bfloat16, jnp.float32

    def scratch(d, dv, both):
        return [
            pltpu.VMEM((4, rows, 2 * d), bf16),
            pltpu.VMEM((2, 4, half, 2 * d + dv) if both else (16, 128), bf16),
            pltpu.VMEM((2 * d, total), bf16),
            pltpu.VMEM((dv, total), bf16),
            pltpu.VMEM((2, dv, total), f32),
            pltpu.VMEM((2, total), f32),
            pltpu.VMEM((2, 8, total), f32),
            pltpu.VMEM((4, total), f32),
            pltpu.VMEM((3, 4, total), f32),
            pltpu.VMEM((4, rows, dv), bf16),
            pltpu.VMEM((3, rows, dv), bf16),
            pltpu.VMEM((2, half, dv), bf16),
            pltpu.VMEM((rows, dv), bf16),
            pltpu.VMEM((mine, 8 * dv), bf16),
        ]
    any_ = pl.BlockSpec(memory_space=pl.ANY)
    vmem = pl.BlockSpec(memory_space=pltpu.VMEM)
    count = 2 * (4 + 2 + 4 + 2 + 4 + 8) + 3 * 9 + 2 * 9
    width = residual.shape[1]
    return pl.pallas_call(
        functools.partial(attention_kernel, rows=rows),
        out_shape=(jax.ShapeDtypeStruct((mine, width), bf16),) * 2,
        in_specs=[pl.BlockSpec(memory_space=pltpu.SMEM), vmem, vmem] + [any_] * 8,
        out_specs=(vmem, vmem),
        scratch_shapes=scratch(64, 128, True) + scratch(128, 256, False) + [
            pltpu.SMEM((3, 2 * 4 * (rows // TQ) * 4 + 1), jnp.int32),
            pltpu.SMEM((12,), jnp.int32),
            pltpu.VMEM((2, rows, TQ), f32),
            pltpu.VMEM((2, rows, TQ), f32),
            pltpu.VMEM((2, 8, TQ), f32),
            pltpu.VMEM((2, 8, TQ), f32),
            pltpu.VMEM((2, rows, TQ), bf16),
            pltpu.SemaphoreType.DMA((count,)),
            pltpu.SemaphoreType.DMA((count,)),
            pltpu.SemaphoreType.DMA((8,)),
            pltpu.VMEM((8 * 384, width), bf16),
            pltpu.VMEM((mine, width), f32),
            pltpu.VMEM((4, half, 512), bf16),
            pltpu.VMEM((4, half, 512), bf16),
        ],
        name="attention",
        cost_estimate=pl.CostEstimate(flops=100 * 10**9, bytes_accessed=10**7, transcendentals=0),
        compiler_params=pltpu.CompilerParams(collective_id=0, has_side_effects=True, vmem_limit_bytes=60 * 2**20),
    )(lam.reshape(-1), residual, gain.reshape(1, -1), out_w, out_n, qn, kn, vn, qw, kw, vw)


def device_of(e):
    return {"z": e // 32, "x": (e // 8) % 4, "y": (e // 2) % 4, "c": e % 2}


def swapped(perm, rows):
    return jnp.dot(perm, rows, preferred_element_type=jnp.float32).astype(jnp.bfloat16)


def to_tiles(perm, block):
    width = block.shape[1] // 16
    stacked = jnp.concatenate([block[:, g * width:(g + 1) * width] for g in range(16)], axis=0)
    return swapped(perm, stacked).reshape(16, 16, width)


def experts_kernel(token_ref, slot_ref, weight_ref, normed_ref, stream_ref, gate_in, up_in, down_in, out_ref,
                   gate_s, up_s, down_s, perm_s, rows_s, stream_s, send_s, got_a, got_b, flat_s, hidden_s, ret_a, ret_b, back_s,
                   weight_sems, send_sems, recv_sems):
    count = 128
    cap = send_s.shape[0] // count
    total = send_s.shape[0]
    part = total // 2
    tokens = normed_ref.shape[0]
    me = ((lax.axis_index("z") * 4 + lax.axis_index("x")) * 4 + lax.axis_index("y")) * 2 + lax.axis_index("c")
    chip, core = me // 2, me % 2
    got, ret = (got_a, got_b), (ret_a, ret_b)
    loads = [
        pltpu.make_async_copy(src.at[0], dst, weight_sems.at[n])
        for n, (src, dst) in enumerate(((gate_in, gate_s), (up_in, up_s), (down_in, down_s)))
    ]
    for c in loads:
        c.start()
    barrier = pltpu.get_barrier_semaphore()

    def greet(k, _):
        pl.semaphore_signal(barrier, inc=1, device_id=device_of((me + k) % count), device_id_type=pl.DeviceIdType.MESH)
        return 0
    lax.fori_loop(1, count, greet, 0)

    r = lax.broadcasted_iota(jnp.int32, (256, 256), 0)
    c = lax.broadcasted_iota(jnp.int32, (256, 256), 1)
    perm_s[...] = jnp.where((r % 16) * 16 + r // 16 == c, 1.0, 0.0).astype(jnp.bfloat16)
    perm = perm_s[...]
    for b in range(tokens // 16):
        s = slice(b * 16, (b + 1) * 16)
        rows_s[s] = to_tiles(perm, normed_ref[s])

    def fill(n, _):
        for u in range(8):
            send_s[n * 8 + u] = rows_s[token_ref[n * 8 + u]]
        return 0
    lax.fori_loop(0, total // 8, fill, 0)
    pl.semaphore_wait(barrier, count - 1)

    def peer(h, j):
        other = (chip + j) % 64
        return other, other * 2 + (core if h == 0 else 1 - core)

    def remote(src, dst, way, n, e):
        return pltpu.make_async_remote_copy(
            src_ref=src, dst_ref=dst, send_sem=send_sems.at[way, n], recv_sem=recv_sems.at[way, n],
            device_id=device_of(e), device_id_type=pl.DeviceIdType.MESH,
        )

    def there(h, j):
        _, e = peer(h, j)
        return remote(send_s.at[pl.ds(e * cap, cap)], got[h].at[pl.ds(chip * cap, cap)], 0, h * 64 + j, e)

    def back(h, j):
        other, e = peer(h, j)
        return remote(ret[h].at[pl.ds(other * cap, cap)], back_s.at[pl.ds(me * cap, cap)], 1, h * 64 + j, e)

    def each(h, act):
        def go(n, _):
            act(h, (n * 37) % 64)
            return 0
        lax.fori_loop(1 - h, 64, go, 0)

    each(0, lambda h, j: there(h, j).start())
    got_a[pl.ds(chip * cap, cap)] = send_s[pl.ds(me * cap, cap)]
    each(1, lambda h, j: there(h, j).start())
    for b in range(tokens // 16):
        s = slice(b * 16, (b + 1) * 16)
        stream_s[s] = to_tiles(perm, stream_ref[s])
    for c in loads:
        c.wait()

    for h in range(2):
        each(h, lambda h, j: there(h, j).wait_recv())

        def flatten(n, _):
            for u in range(4):
                at = pl.multiple_of((n * 4 + u) * 16, 16)
                turned = swapped(perm, got[h][pl.ds(at, 16)].reshape(256, 128))
                for g in range(16):
                    flat_s[pl.ds(at, 16), g * 128:(g + 1) * 128] = turned[g * 16:(g + 1) * 16]
            return 0
        lax.fori_loop(0, part // 64, flatten, 0)

        def first(n, _):
            at = pl.ds(pl.multiple_of(n * 256, 256), 256)
            gate = jnp.dot(flat_s[...], gate_s[:, at], preferred_element_type=jnp.float32)
            up = jnp.dot(flat_s[...], up_s[:, at], preferred_element_type=jnp.float32)
            hidden_s[:, at] = (gate * jax.nn.sigmoid(gate) * up).astype(jnp.bfloat16)
            return 0
        lax.fori_loop(0, hidden_s.shape[1] // 256, first, 0)

        def second(n, _):
            at = pl.ds(pl.multiple_of(n * 256, 256), 256)
            flat_s[:, at] = jnp.dot(hidden_s[...], down_s[:, at], preferred_element_type=jnp.float32).astype(jnp.bfloat16)
            return 0
        lax.fori_loop(0, flat_s.shape[1] // 256, second, 0)

        def unflatten(n, _):
            for u in range(4):
                at = pl.ds(pl.multiple_of((n * 4 + u) * 16, 16), 16)
                ret[h][at] = to_tiles(perm, flat_s[at, :])
            return 0
        lax.fori_loop(0, part // 64, unflatten, 0)
        each(h, lambda h, j: back(h, j).start())
    back_s[pl.ds(me * cap, cap)] = ret_a[pl.ds(chip * cap, cap)]
    for h in range(2):
        each(h, lambda h, j: back(h, j).wait_recv())

    def combine(n, _):
        for u in range(4):
            t = n * 4 + u
            summed = weight_ref[2 * t] * back_s[slot_ref[2 * t]].astype(jnp.float32)
            summed = summed + weight_ref[2 * t + 1] * back_s[slot_ref[2 * t + 1]].astype(jnp.float32)
            rows_s[t] = (stream_s[t].astype(jnp.float32) + summed).astype(jnp.bfloat16)
        return 0
    lax.fori_loop(0, tokens // 4, combine, 0)
    for b in range(tokens // 16):
        s = slice(b * 16, (b + 1) * 16)
        turned = swapped(perm, rows_s[s].reshape(256, 128))
        for g in range(16):
            out_ref[s, g * 128:(g + 1) * 128] = turned[g * 16:(g + 1) * 16]
    for h in range(2):
        each(h, lambda h, j: there(h, j).wait_send())
        each(h, lambda h, j: back(h, j).wait_send())


def experts(token_of_slot, slot_of_token, weight, normed, stream, gate, up, down):
    tokens, width = normed.shape
    slots = token_of_slot.shape[0]
    inner = gate.shape[2]
    smem = pl.BlockSpec(memory_space=pltpu.SMEM)
    vmem = pl.BlockSpec(memory_space=pltpu.VMEM)
    any_ = pl.BlockSpec(memory_space=pl.ANY)
    bf16 = jnp.bfloat16
    return pl.pallas_call(
        experts_kernel,
        out_shape=jax.ShapeDtypeStruct((tokens, width), bf16),
        in_specs=[smem] * 3 + [vmem] * 2 + [any_] * 3,
        out_specs=vmem,
        scratch_shapes=[
            pltpu.VMEM((width, inner), bf16),
            pltpu.VMEM((width, inner), bf16),
            pltpu.VMEM((inner, width), bf16),
            pltpu.VMEM((256, 256), bf16),
            pltpu.VMEM((tokens, 16, width // 16), bf16),
            pltpu.VMEM((tokens, 16, width // 16), bf16),
            pltpu.VMEM((slots, 16, width // 16), bf16),
            pltpu.VMEM((slots // 2, 16, width // 16), bf16),
            pltpu.VMEM((slots // 2, 16, width // 16), bf16),
            pltpu.VMEM((slots // 2, width), bf16),
            pltpu.VMEM((slots // 2, inner), bf16),
            pltpu.VMEM((slots // 2, 16, width // 16), bf16),
            pltpu.VMEM((slots // 2, 16, width // 16), bf16),
            pltpu.VMEM((slots, 16, width // 16), bf16),
            pltpu.SemaphoreType.DMA((3,)),
            pltpu.SemaphoreType.DMA((2, 128)),
            pltpu.SemaphoreType.DMA((2, 128)),
        ],
        name="experts",
        cost_estimate=pl.CostEstimate(flops=50 * 10**9, bytes_accessed=2 * 10**7, transcendentals=0),
        compiler_params=pltpu.CompilerParams(collective_id=1, has_side_effects=True, vmem_limit_bytes=60 * 2**20),
    )(token_of_slot, slot_of_token, weight, normed, stream, gate, up, down)


def shards(
    query_wide,
    key_wide,
    value_wide,
    query_narrow,
    key_narrow,
    value_narrow,
    mix_lambda,
    residual_in,
    out_wide,
    out_narrow,
    ffn_gain,
    expert_ids,
    expert_weights,
    gate_weight,
    up_weight,
    down_weight,
):
    tok_count, local_heads, _ = query_wide.shape
    stream, normed = attention(
        query_wide, key_wide, value_wide, query_narrow, key_narrow, value_narrow, mix_lambda,
        residual_in, out_wide, out_narrow, ffn_gain,
    )
    tp_size = lax.axis_size(TP)
    local_rows = tok_count // tp_size
    experts_all = lax.axis_size(SP) * tp_size
    capacity = max(2, 4 * local_rows // experts_all)
    flat_expert = expert_ids.reshape(-1)
    expert_hot = (flat_expert[:, None] == jnp.arange(experts_all, dtype=jnp.int32)[None, :]).astype(
        jnp.int32
    )
    slot_rank = jnp.sum((jnp.cumsum(expert_hot, axis=0) - 1) * expert_hot, axis=1)
    flat_slot = flat_expert * capacity + slot_rank
    slot_ids = jnp.arange(experts_all * capacity, dtype=jnp.int32)
    placed = slot_ids[:, None] == flat_slot[None, :]
    token = jnp.arange(2 * local_rows, dtype=jnp.int32) // 2
    token_of_slot = jnp.max(jnp.where(placed, token[None, :], 0), axis=1)
    return experts(
        token_of_slot, flat_slot, expert_weights.reshape(-1), normed, stream, gate_weight, up_weight, down_weight
    )


def solution(mesh):
    finer = Mesh(mesh.devices.reshape(4, 4, 4, 2), ("z", "x", "y", "c"))
    placed = (
        P(SP, TP, None),
        P(SP, TP, None),
        P(SP, TP, None),
        P(SP, TP, None),
        P(SP, TP, None),
        P(SP, TP, None),
        P(None, TP),
        P(SP_TP, None),
        P(TP, None),
        P(TP, None),
        P(),
        P(SP_TP, None),
        P(SP_TP, None),
        P(SP_TP, None, None),
        P(SP_TP, None, None),
        P(SP_TP, None, None),
    )
    return jax.shard_map(
        shards, mesh=finer, in_specs=placed, out_specs=P(SP_TP, None), check_vma=False
    )
```
